256 devices in a mesh: kv: 32 (over z, x), tp: 8 (over y, core).
Axes of the slice: x: 4, y: 4, z: 8, core: 2. Of those that a mesh axis runs over, the one named last changes fastest.
Arguments:
- inputs: bfloat16 [4, 8192, 2048], P(None, 'kv'), may hold values from -40 to 40
- query_weight: bfloat16 [2048, 2048], P(None, 'tp'), may hold values from -0.125 to 0.125
- key_weight: bfloat16 [2048, 1024], P(None, 'tp'), may hold values from -0.125 to 0.125
- value_weight: bfloat16 [2048, 1024], P(None, 'tp'), may hold values from -0.125 to 0.125
- out_weight: bfloat16 [2048, 2048], P('tp'), may hold values from -1 to 1
- chosen: int32 [4, 128, 32], P(None, 'kv'), may hold values from 0 to 127, as said below
- lengths: int32 [4], replicated, may hold values from 1 to 8192, 12288 in all
Outputs:
- mixed: bfloat16 [4, 8192, 2048], P(None, 'kv', 'tp')
The draws below stay inside these ranges and needn't reach their ends.
Inputs may be any that keep to these rules, and one draw needn't show every extreme that they name: chosen[b, q, 0] = q; every entry names a block of the same sequence at or before q; entries may repeat. Over the query blocks of positions k * 256 to (k+1) * 256 - 1 of all sequences, the named blocks that lie in another span of 256 positions number at most 3 distinct blocks for each other span, and 3 is reached.
All inputs are finite; a program needn't handle non-finite values.
Results may differ from the reference program's by a relative error of at most 0.014.
The reference program's roundings to bfloat16 on the way count: a program that leaves them out, or rounds other values in their place, can miss the bound.
Values may be sent and summed in bfloat16 or wider, within the bound.
A program may use at most 128 MiB of HBM per device.

```python
import math
import jax
import jax.numpy as jnp
import numpy as np
from jax import lax

D = 2048
HEADS = 16
KV_HEADS = 8
HD = 128
KB = 64
TOPK = 32
CAP = 3
BATCH = 4
SEQ_DEV = 256
SEQ = 8192
NB = 128
N_TP = 8


def draw_inputs(key, part):
    key_base = jax.random.fold_in(jax.random.fold_in(key, 3), 0)
    entries = jax.random.normal(key_base, (BATCH, SEQ, D), jnp.float32)
    return jnp.clip(entries, -40.0, 40.0).astype(jnp.bfloat16)


def draw_chosen(key, part):
    per_dev = SEQ_DEV // KB
    ndevices = NB // per_dev
    owned = BATCH * per_dev
    key_count, key_rank, key_order = jax.random.split(jax.random.fold_in(key, 7), 3)
    receiver = jnp.arange(ndevices, dtype=jnp.int32)[:, None]
    sender = jnp.arange(ndevices, dtype=jnp.int32)[None, :]
    counts = jax.random.randint(key_count, (ndevices, ndevices), 1, CAP + 1)
    counts = jnp.where(sender == receiver - 1, CAP, counts)
    counts = jnp.where(sender < receiver, counts, 0)
    local_ids = jnp.arange(owned, dtype=jnp.int32)
    noise = jax.random.randint(key_rank, (ndevices, ndevices, owned), 0, 1 << 20) * owned + local_ids
    ranks = jnp.argsort(jnp.argsort(noise, axis=-1), axis=-1)
    picked = ranks < counts[:, :, None]
    order_noise = jax.random.randint(key_order, (ndevices, ndevices), 0, 1 << 20) * ndevices + sender
    priority = jnp.argsort(jnp.argsort(order_noise, axis=-1), axis=-1) + 2
    priority = jnp.where(sender == receiver - ndevices // 2, 1, priority)
    priority = jnp.where(sender == receiver - 1, 0, priority)
    seq_of = local_ids // per_dev
    global_block = sender[:, :, None] * per_dev + (local_ids % per_dev)[None, None, :]
    big_score = (ndevices + 4) * owned
    seq_range = jnp.arange(BATCH, dtype=jnp.int32)
    in_seq = picked[:, None, :, :] & (seq_of[None, None, None, :] == seq_range[None, :, None, None])
    scored = jnp.where(in_seq, priority[:, None, :, None] * owned + local_ids[None, None, None, :], big_score)
    scored = scored.reshape(ndevices, BATCH, ndevices * owned)
    sorted_idx = jnp.argsort(scored, axis=-1)
    pool_size = jnp.sum(in_seq.reshape(ndevices, BATCH, ndevices * owned).astype(jnp.int32), axis=-1)
    pool_blocks = jnp.take_along_axis(jnp.broadcast_to(global_block.reshape(1, 1, ndevices * owned), (ndevices, BATCH, ndevices * owned)), sorted_idx, axis=-1)
    local_row = jnp.arange(per_dev, dtype=jnp.int32)[:, None]
    slot_col = jnp.arange(TOPK, dtype=jnp.int32)[None, :]
    base_count = local_row * (TOPK - 1) - local_row * (local_row - 1) // 2
    counter = base_count + slot_col - 1 - local_row
    safe_size = jnp.maximum(pool_size, 1)
    pool_pick = jnp.take_along_axis(pool_blocks, counter.reshape(1, 1, -1) % safe_size[:, :, None], axis=-1)
    pool_pick = pool_pick.reshape(ndevices, BATCH, per_dev, TOPK)
    own_block = jnp.arange(ndevices, dtype=jnp.int32)[:, None, None, None] * per_dev + local_row[None, None, :, :] + 0 * slot_col[None, None, :, :]
    earlier = own_block - local_row[None, None, :, :] + slot_col[None, None, :, :] - 1
    result = jnp.where(pool_size[:, :, None, None] > 0, pool_pick, own_block)
    result = jnp.where((slot_col >= 1) & (slot_col <= local_row), earlier, result)
    result = jnp.where(slot_col == 0, own_block, result)
    return jnp.transpose(result, (1, 0, 2, 3)).reshape(BATCH, NB, TOPK).astype(jnp.int32)


def level_of(stream_key, dims, cuts, smallest, largest):
    level = 1.0
    for dim, parts in cuts:
        steps = jax.random.uniform(jax.random.fold_in(jax.random.fold_in(stream_key, 6), dim), (parts,), jnp.float32, smallest / len(cuts), largest / len(cuts))
        level = level * jnp.repeat(jnp.exp(steps), dims[dim] // parts).reshape((-1,) + (1,) * (len(dims) - 1 - dim))
    return level


def profile(count, total, reach, lean):
    portions = [(1 << 20) // math.isqrt(grade ** lean) + 1 for grade in range(2, count + 1)]
    surplus, given = total - reach - (count - 1), [1] * (count - 1)
    while surplus > 0:
        candidates = [i for i in range(count - 1) if given[i] < reach]
        mass, budget = sum([portions[i] for i in candidates]), surplus
        for i in candidates:
            addition = min(reach - given[i], max(1, budget * portions[i] // mass), surplus)
            given[i] = given[i] + addition
            surplus = surplus - addition
    return np.array([reach] + given)


def uneven(key, amount, total, bound, slope):
    if amount == 2:
        one = jax.random.randint(key, (), max(1, total - bound), min(bound, total - 1) + 1)
        return jnp.stack([one, total - one])
    tallies = jnp.asarray(profile(amount, total, bound, slope), jnp.int32)
    pairs = (amount - 1) // 2
    source_of, taker = tallies[1:1 + 2 * pairs:2], tallies[2:2 + 2 * pairs:2]
    margin = jnp.minimum(source_of - 1, bound - taker)
    moved = jax.random.randint(jax.random.fold_in(key, 1), (pairs,), 0, 1 << 20) % (margin + 1)
    tallies = tallies.at[1:1 + 2 * pairs:2].set(source_of - moved).at[2:2 + 2 * pairs:2].set(taker + moved)
    return tallies[jax.random.permutation(jax.random.fold_in(key, 2), amount)]


def gaussian(stream_key, extent, spread, bound, pieces=(), kind=jnp.bfloat16):
    array = jax.random.normal(stream_key, extent, jnp.float32) * spread
    if len(pieces) > 0:
        array = level_of(stream_key, extent, pieces, -0.22, 0.18) * array
    return jnp.clip(array, min=-bound, max=bound).astype(kind)


def setup_inputs(seed: int = 0) -> dict:
    seeds = jax.random.split(jax.random.key(seed), 8)
    return {
        "inputs": draw_inputs(jax.random.fold_in(seeds[7], 71), 0),
        "query_weight": gaussian(seeds[1], (D, HEADS * HD), D ** -0.5, 0.125, ((1, 8),)),
        "key_weight": gaussian(seeds[2], (D, KV_HEADS * HD), D ** -0.5, 0.125, ((1, 8),)),
        "value_weight": gaussian(seeds[3], (D, KV_HEADS * HD), D ** -0.5, 0.125, ((1, 8),)),
        "out_weight": gaussian(seeds[4], (HEADS * HD, D), (HEADS * HD // 64) ** -0.5, 1.0, ((0, 8),)),
        "chosen": draw_chosen(jax.random.fold_in(seeds[7], 71), 0),
        "lengths": uneven(seeds[6], BATCH, SEQ + SEQ // 2, SEQ, 2).astype(jnp.int32),
    }


def unique_slots(chosen_rows):
    order = jnp.arange(TOPK, dtype=jnp.int32)
    repeated = jnp.any((chosen_rows[..., :, None] == chosen_rows[..., None, :]) & (order[:, None] > order[None, :]), axis=-1)
    return jnp.repeat(jnp.logical_not(repeated), KB, axis=-1)


def attend(queries, key_sets, value_sets, key_pos, unique_key, query_pos, live_length):
    scores = jnp.einsum("nqkgd,npkd->nkgqp", queries.astype(jnp.float32), key_sets.astype(jnp.float32)) * (HD ** -0.5)
    allowed = (key_pos[:, None, :] <= query_pos[:, :, None]) & (key_pos[:, None, :] < live_length) & unique_key[:, None, :]
    allowed = allowed | (key_pos[:, None, :] == query_pos[:, :, None])
    scores = jnp.where(allowed[:, None, None], scores, -jnp.inf)
    highest = jnp.max(scores, axis=-1, keepdims=True)
    raised = jnp.exp(scores - highest)
    weights = (raised / jnp.sum(raised, axis=-1, keepdims=True)).astype(jnp.bfloat16)
    combined = jnp.einsum("nkgqp,npkd->nqkgd", weights.astype(jnp.float32), value_sets.astype(jnp.float32))
    living = (query_pos < live_length)[:, :, None, None, None]
    return jnp.where(living, combined, 0.0).astype(jnp.bfloat16)


def reference(inputs, query_weight, key_weight, value_weight, out_weight, chosen, lengths):
    per_group = HEADS // KV_HEADS
    flat_rows = inputs.reshape(BATCH * SEQ, D)
    queries = jnp.dot(flat_rows, query_weight, preferred_element_type=jnp.float32).astype(jnp.bfloat16)
    queries = queries.reshape(BATCH, NB, KB, KV_HEADS, per_group, HD)
    key_rows = jnp.dot(flat_rows, key_weight, preferred_element_type=jnp.float32).astype(jnp.bfloat16)
    key_rows = key_rows.reshape(BATCH, NB, KB, KV_HEADS, HD)
    value_rows = jnp.dot(flat_rows, value_weight, preferred_element_type=jnp.float32).astype(jnp.bfloat16)
    value_rows = value_rows.reshape(BATCH, NB, KB, KV_HEADS, HD)
    offsets = jnp.arange(KB, dtype=jnp.int32)

    def one_block(block_pair):
        seq_index, block_id = block_pair
        names = chosen[seq_index, block_id]
        key_sets = key_rows[seq_index][names].reshape(1, TOPK * KB, KV_HEADS, HD)
        value_sets = value_rows[seq_index][names].reshape(1, TOPK * KB, KV_HEADS, HD)
        key_pos = (names[:, None] * KB + offsets[None, :]).reshape(1, TOPK * KB)
        query_pos = (block_id * KB + offsets)[None, :]
        unique_key = unique_slots(names)[None, :]
        result = attend(queries[seq_index, block_id][None], key_sets, value_sets, key_pos, unique_key, query_pos, lengths[seq_index])
        return result[0]

    seq_ids = jnp.repeat(jnp.arange(BATCH, dtype=jnp.int32), NB)
    block_ids = jnp.tile(jnp.arange(NB, dtype=jnp.int32), BATCH)
    attended = lax.map(one_block, (seq_ids, block_ids)).reshape(BATCH * SEQ, HEADS * HD)
    group_width = HEADS * HD // N_TP
    summed = jnp.zeros((BATCH * SEQ, D), jnp.float32)
    for group_id in range(N_TP):
        partial_value = jnp.dot(attended[:, group_id * group_width:(group_id + 1) * group_width],
                          out_weight[group_id * group_width:(group_id + 1) * group_width],
                          preferred_element_type=jnp.float32).astype(jnp.bfloat16)
        summed = summed + lax.optimization_barrier(partial_value).astype(jnp.float32)
    return summed.astype(jnp.bfloat16).reshape(BATCH, SEQ, D)
```

```python
import jax
import jax.numpy as jnp
from jax import lax
from jax.experimental import pallas as pl
from jax.experimental.pallas import tpu as pltpu
from jax.sharding import PartitionSpec as P

HD = 128
KB = 64
TOPK = 32
SEQS = 4
SPAN = 256
MODEL = 2048
NZ, NX, NY = 8, 4, 4
NTP = 8
REACH = (7, 5, 3, 2)
CHUNK = 512
MESH = pl.DeviceIdType.MESH
ANY = pl.BlockSpec(memory_space=pl.ANY)
SMEM = pl.BlockSpec(memory_space=pltpu.SMEM)
VMEM = pl.BlockSpec(memory_space=pltpu.VMEM)


def sequence_of(slot, lengths):
    size = [lengths[b] for b in range(SEQS)]
    found = jnp.int32(0)
    for b in range(SEQS):
        rank = jnp.int32(0)
        for o in range(SEQS):
            if o < b:
                rank += (size[o] >= size[b]).astype(jnp.int32)
            elif o > b:
                rank += (size[o] > size[b]).astype(jnp.int32)
        found += jnp.where(rank == slot, b, 0)
    return found


def project_kernel(lengths, x, query_w, key_w, value_w, q_out, kv_out, weights):
    @pl.when(pl.program_id(0) == 0)
    def _():
        weights[:, :HD] = key_w[...]
        weights[:, HD:] = value_w[...]

    rows = x[0]
    kv_out[0] = jnp.dot(rows, weights[...], preferred_element_type=jnp.float32).astype(jnp.bfloat16)
    q_out[0] = jnp.dot(rows, query_w[...], preferred_element_type=jnp.float32).astype(jnp.bfloat16)


def project(lengths, inputs, query_weight, key_weight, value_weight):
    once = dict(pipeline_mode=pl.Buffered(1))
    out = jax.ShapeDtypeStruct((SEQS, SPAN, 2 * HD), jnp.bfloat16)
    block = pl.BlockSpec((1, SPAN, 2 * HD), lambda j, lens: (j, 0, 0))
    return pl.pallas_call(
        project_kernel,
        name="project",
        out_shape=(out, out),
        grid_spec=pltpu.PrefetchScalarGridSpec(
            num_scalar_prefetch=1,
            grid=(SEQS,),
            in_specs=[
                pl.BlockSpec((1, SPAN, MODEL), lambda j, lens: (sequence_of(j, lens), 0, 0)),
                pl.BlockSpec((MODEL, 2 * HD), lambda j, lens: (0, 0), **once),
                pl.BlockSpec((MODEL, HD), lambda j, lens: (0, 0), **once),
                pl.BlockSpec((MODEL, HD), lambda j, lens: (0, 0), **once),
            ],
            out_specs=(block, block),
            scratch_shapes=[pltpu.VMEM((MODEL, 2 * HD), jnp.bfloat16)],
        ),
    )(lengths, inputs, query_weight, key_weight, value_weight)


def spread_kernel(reach, own, out_w, cache, columns, recv, up_sem, right_sem, left_sem,
                  pass_right, pass_left, w_send, w_recv):
    kv, tp = lax.axis_index("kv"), lax.axis_index("tp")
    z, x = kv // NX, kv % NX
    up = {"kv": ((z + 1) % NZ) * NX + x}
    down = {"kv": ((z + NZ - 1) % NZ) * NX + x}
    right = {"kv": z * NX + (x + 1) % NX}
    left = {"kv": z * NX + (x + NX - 1) % NX}
    x_right, x_left, x_far = (x + 1) % NX, (x + NX - 1) % NX, (x + 2) % NX
    half = SPAN // 2

    barrier = pltpu.get_barrier_semaphore()
    for d in (up, down, right, left):
        pl.semaphore_signal(barrier, inc=1, device_id=d, device_id_type=MESH)
    for d in range(1, NTP):
        pl.semaphore_signal(barrier, inc=1, device_id={"tp": (tp + d) % NTP}, device_id_type=MESH)
    pl.semaphore_wait(barrier, 4 + NTP - 1)

    def piece(slot, owner_z, owner_x, h):
        first = pl.multiple_of((owner_z * NX + owner_x) * SPAN + h * half, half)
        return cache.at[slot, pl.ds(first, half)]

    def send(src, dst, sem, slot, owner_z, owner_x, h, device):
        return pltpu.make_async_remote_copy(
            src_ref=src, dst_ref=dst, send_sem=sem,
            recv_sem=recv.at[slot, owner_z * NX + owner_x, h],
            device_id=device, device_id_type=MESH)

    def arrived(slot, owner_z, owner_x, h):
        here = piece(slot, owner_z, owner_x, h)
        send(here, here, up_sem.at[slot, 0, h], slot, owner_z, owner_x, h, right).wait_recv()

    def column(t, source):
        w = z - t
        for slot in range(SEQS):
            @pl.when(z <= reach[slot])
            def _(slot=slot):
                for h in range(2):
                    there = piece(slot, w, x, h)
                    if source is None:
                        arrived(slot, w, x, h)
                        src = there
                    else:
                        src = source.at[slot, pl.ds(h * half, half)]

                    @pl.when(z + 1 <= reach[slot])
                    def _():
                        send(src, there, up_sem.at[slot, t, h], slot, w, x, h, up).start()

                    send(src, there, right_sem.at[slot, t, h], slot, w, x, h, right).start()
                    send(src, there, left_sem.at[slot, t, h], slot, w, x, h, left).start()

    def around(t):
        w = z - t
        for slot in range(SEQS):
            @pl.when(z <= reach[slot])
            def _(slot=slot):
                arrived(slot, w, x_left, 0)
                there = piece(slot, w, x_left, 0)
                send(there, there, pass_right.at[slot, t], slot, w, x_left, 0, right).start()
                arrived(slot, w, x_right, 1)
                there = piece(slot, w, x_right, 1)
                send(there, there, pass_left.at[slot, t], slot, w, x_right, 1, left).start()

    def finish(t):
        w = z - t
        for slot in range(SEQS):
            @pl.when(z <= reach[slot])
            def _(slot=slot):
                arrived(slot, w, x_left, 1)
                arrived(slot, w, x_right, 0)
                for h in range(2):
                    arrived(slot, w, x_far, h)
                    here = piece(slot, w, x, h)

                    @pl.when(z + 1 <= reach[slot])
                    def _():
                        send(here, here, up_sem.at[slot, t, h], slot, w, x, h, up).wait_send()

                    send(here, here, right_sem.at[slot, t, h], slot, w, x, h, right).wait_send()
                    send(here, here, left_sem.at[slot, t, h], slot, w, x, h, left).wait_send()
                here = piece(slot, w, x, 0)
                send(here, here, pass_right.at[slot, t], slot, w, x, 0, right).wait_send()
                send(here, here, pass_left.at[slot, t], slot, w, x, 0, left).wait_send()

    def column_copy(d):
        peer = (tp + d) % NTP
        first = pl.multiple_of(peer * SPAN, SPAN)
        return pltpu.make_async_remote_copy(
            src_ref=out_w.at[:, pl.ds(first, SPAN)], dst_ref=columns.at[tp],
            send_sem=w_send.at[d - 1], recv_sem=w_recv.at[d - 1],
            device_id={"tp": peer}, device_id_type=MESH)

    column(0, own)
    for d in range(1, NTP):
        column_copy(d).start()

    @pl.loop(1, NZ + 1)
    def _(t):
        @pl.when(t <= z)
        def _():
            column(t, None)

        @pl.when(t - 1 <= z)
        def _():
            around(t - 1)

    @pl.loop(0, NZ)
    def _(t):
        @pl.when(t <= z)
        def _():
            finish(t)

    for d in range(1, NTP):
        column_copy(d).wait()


def spread(reach, own, out_weight):
    dma = pltpu.SemaphoreType.DMA
    return pl.pallas_call(
        lambda *refs: spread_kernel(reach, *refs),
        name="spread",
        out_shape=(
            jax.ShapeDtypeStruct((SEQS, NZ * NX * SPAN, 2 * HD), jnp.bfloat16),
            jax.ShapeDtypeStruct((NTP, SPAN, SPAN), jnp.bfloat16),
        ),
        in_specs=[ANY, ANY],
        out_specs=(ANY, ANY),
        scratch_shapes=[
            dma((SEQS, NZ * NX, 2)),
            dma((SEQS, NZ, 2)),
            dma((SEQS, NZ, 2)),
            dma((SEQS, NZ, 2)),
            dma((SEQS, NZ)),
            dma((SEQS, NZ)),
            dma((NTP - 1,)),
            dma((NTP - 1,)),
        ],
        compiler_params=pltpu.CompilerParams(collective_id=0, has_side_effects=True),
    )(own, out_weight)


def attend_kernel(lengths, chosen, q, own, cache, out, keys, scores, seen, count, again, sems):
    kv = lax.axis_index("kv")
    tasks = SEQS * (SPAN // KB)
    out[...] = jnp.zeros_like(out)
    keys[...] = jnp.zeros_like(keys)

    @pl.loop(0, NZ * NX * (SPAN // KB))
    def _(i):
        seen[i] = -1

    def place(task):
        return task // 4, task % 4

    def fetch(task):
        slot, i = place(task)
        b = sequence_of(slot, lengths)
        buffer = task % 2
        count[task] = 0

        @pl.when((kv * 4 + i) * KB < lengths[b])
        def _():
            def entry(e, found):
                n, repeats = found
                block = chosen[b, i, e]
                fresh = seen[block] != task

                @pl.when(fresh)
                def _():
                    seen[block] = task
                    to = keys.at[buffer, pl.ds(pl.multiple_of(n * KB, KB), KB)]
                    near = block // 4 == kv

                    @pl.when(near)
                    def _():
                        row = pl.multiple_of(block % 4 * KB, KB)
                        pltpu.make_async_copy(own.at[slot, pl.ds(row, KB)], to, sems.at[buffer]).start()

                    @pl.when(jnp.logical_not(near))
                    def _():
                        row = pl.multiple_of(block * KB, KB)
                        pltpu.make_async_copy(cache.at[slot, pl.ds(row, KB)], to, sems.at[buffer]).start()

                same = (block == kv * 4 + i).astype(jnp.int32)
                return n + fresh.astype(jnp.int32), repeats + same

            n, repeats = lax.fori_loop(0, TOPK, entry, (jnp.int32(0), jnp.int32(-1)))
            count[task] = n
            again[task] = repeats

    def compute(task):
        slot, i = place(task)
        buffer = task % 2
        n = count[task]

        @pl.when(n > 0)
        def _():
            live = lengths[sequence_of(slot, lengths)]

            @pl.loop(0, n)
            def _(e):
                to = keys.at[buffer, pl.ds(0, KB)]
                pltpu.make_async_copy(own.at[slot, pl.ds(0, KB)], to, sems.at[buffer]).wait()

            rows = pl.ds(pl.multiple_of(i * KB, KB), KB)
            both = q[slot, rows, :]
            stacked = jnp.concatenate([both[:, :HD], both[:, HD:]], axis=0)
            chunks = (n * KB + CHUNK - 1) // CHUNK
            row = lax.broadcasted_iota(jnp.int32, (2 * KB, CHUNK), 0) % KB
            lane = lax.broadcasted_iota(jnp.int32, (2 * KB, CHUNK), 1)

            def score(c, highest):
                part = keys[buffer, pl.ds(pl.multiple_of(c * CHUNK, CHUNK), CHUNK), :HD]
                s = lax.dot_general(stacked, part, (((1,), (1,)), ((), ())),
                                    preferred_element_type=jnp.float32) * (HD ** -0.5)
                col = lane + c * CHUNK
                limit = jnp.where(col < KB, row, n * KB - 1)
                allowed = col <= limit
                s = jnp.where(allowed, s, -jnp.inf)
                scores[c] = s
                return jnp.maximum(highest, jnp.max(s, axis=-1, keepdims=True))

            highest = lax.fori_loop(0, chunks, score, jnp.full((2 * KB, 1), -jnp.inf, jnp.float32))

            def raise_(c, total):
                e = jnp.exp(scores[c] - highest)
                scores[c] = e
                return total + jnp.sum(e, axis=-1, keepdims=True)

            total = lax.fori_loop(0, chunks, raise_, jnp.zeros((2 * KB, 1), jnp.float32))
            repeats = again[task].astype(jnp.float32)
            at = lax.broadcasted_iota(jnp.int32, (2 * KB, HD), 0) % KB
            diagonal = lax.broadcasted_iota(jnp.int32, (2 * KB, HD), 1) == at
            self_score = jnp.where(diagonal, scores[0, :, :HD], 0.0)
            total += repeats * jnp.sum(self_score, axis=-1, keepdims=True)
            share = 1.0 / total
            self_weight = (self_score * share).astype(jnp.bfloat16)
            start = repeats * jnp.dot(self_weight, keys[buffer, :HD, HD:],
                                      preferred_element_type=jnp.float32)

            def combine(c, acc):
                weight = (scores[c] * share).astype(jnp.bfloat16)
                part = keys[buffer, pl.ds(pl.multiple_of(c * CHUNK, CHUNK), CHUNK), HD:]
                return acc + jnp.dot(weight, part, preferred_element_type=jnp.float32)

            acc = lax.fori_loop(0, chunks, combine, start)
            pos = (kv * 4 + i) * KB + at
            acc = jnp.where(pos < live, acc, 0.0).astype(jnp.bfloat16)
            out[slot, rows, :HD] = acc[:KB]
            out[slot, rows, HD:] = acc[KB:]

    fetch(jnp.int32(0))

    @pl.loop(0, tasks)
    def _(task):
        @pl.when(task + 1 < tasks)
        def _():
            fetch(task + 1)

        compute(task)


def attend(lengths, chosen, q, own, cache):
    return pl.pallas_call(
        attend_kernel,
        name="attend",
        out_shape=jax.ShapeDtypeStruct((SEQS, SPAN, 2 * HD), jnp.bfloat16),
        in_specs=[SMEM, SMEM, VMEM, ANY, ANY],
        out_specs=VMEM,
        scratch_shapes=[
            pltpu.VMEM((2, TOPK * KB, 2 * HD), jnp.bfloat16),
            pltpu.VMEM((TOPK * KB // CHUNK, 2 * KB, CHUNK), jnp.float32),
            pltpu.SMEM((NZ * NX * (SPAN // KB),), jnp.int32),
            pltpu.SMEM((SEQS * (SPAN // KB),), jnp.int32),
            pltpu.SMEM((SEQS * (SPAN // KB),), jnp.int32),
            pltpu.SemaphoreType.DMA((2,)),
        ],
    )(lengths, chosen, q, own, cache)


def collect_kernel(reach, own, groups, next_recv, prev_recv, core_recv, next_send, prev_send,
                   next_pass, prev_pass, core_send):
    kv, tp = lax.axis_index("kv"), lax.axis_index("tp")
    z = kv // NX
    y, core = tp // 2, tp % 2
    y_next, y_prev, y_far = (y + 1) % NY, (y + NY - 1) % NY, (y + 2) % NY
    after, before = {"tp": y_next * 2 + core}, {"tp": y_prev * 2 + core}
    partner = {"tp": y * 2 + 1 - core}
    half = SPAN // 2

    barrier = pltpu.get_barrier_semaphore()
    for d in (after, before, partner):
        pl.semaphore_signal(barrier, inc=1, device_id=d, device_id_type=MESH)
    pl.semaphore_wait(barrier, 3)

    def piece(owner_y, owner_core, slot, h):
        return groups.at[owner_y * 2 + owner_core, slot, pl.ds(h * half, half)]

    def copy(src, dst, send_sem, recv_sem, device):
        return pltpu.make_async_remote_copy(
            src_ref=src, dst_ref=dst, send_sem=send_sem, recv_sem=recv_sem,
            device_id=device, device_id_type=MESH)

    def mine(slot, h):
        return own.at[slot, pl.ds(h * half, half)]

    def to_next(slot, h):
        return copy(mine(slot, h), piece(y, core, slot, h), next_send.at[slot, h],
                    next_recv.at[0, slot, h], after)

    def to_prev(slot, h):
        return copy(mine(slot, h), piece(y, core, slot, h), prev_send.at[slot, h],
                    prev_recv.at[0, slot, h], before)

    def on_next(slot):
        here = piece(y_prev, core, slot, 0)
        return copy(here, here, next_pass.at[slot], next_recv.at[1, slot, 0], after)

    def on_prev(slot):
        here = piece(y_next, core, slot, 1)
        return copy(here, here, prev_pass.at[slot], prev_recv.at[1, slot, 1], before)

    def across(far, owner_y, slot, h, src=None):
        here = piece(owner_y, core, slot, h)
        return copy(here if src is None else src, here, core_send.at[far, slot, h],
                    core_recv.at[far, slot, h], partner)

    def each(body):
        for slot in range(SEQS):
            @pl.when(z <= reach[slot])
            def _(slot=slot):
                body(slot)

    def begin(slot):
        to_next(slot, 0).start()
        to_prev(slot, 1).start()
        to_next(slot, 1).start()
        to_prev(slot, 0).start()
        for h in range(2):
            across(0, y, slot, h, mine(slot, h)).start()

    def relay(slot):
        to_next(slot, 0).wait_recv()
        on_next(slot).start()
        across(1, y_prev, slot, 0).start()
        to_prev(slot, 1).wait_recv()
        on_prev(slot).start()
        across(2, y_next, slot, 1).start()
        to_next(slot, 1).wait_recv()
        across(1, y_prev, slot, 1).start()
        to_prev(slot, 0).wait_recv()
        across(2, y_next, slot, 0).start()

    def far(slot):
        on_next(slot).wait_recv()
        across(3, y_far, slot, 0).start()
        on_prev(slot).wait_recv()
        across(3, y_far, slot, 1).start()

    def finish(slot):
        for h in range(2):
            to_next(slot, h).wait_send()
            to_prev(slot, h).wait_send()
            across(0, y, slot, h).wait()
            across(1, y_prev, slot, h).wait()
            across(2, y_next, slot, h).wait()
            across(3, y_far, slot, h).wait()
        on_next(slot).wait_send()
        on_prev(slot).wait_send()

    each(begin)
    each(relay)
    each(far)
    each(finish)


def collect(reach, own):
    dma = pltpu.SemaphoreType.DMA
    return pl.pallas_call(
        lambda *refs: collect_kernel(reach, *refs),
        name="collect",
        out_shape=jax.ShapeDtypeStruct((NTP, SEQS, SPAN, 2 * HD), jnp.bfloat16),
        in_specs=[ANY],
        out_specs=ANY,
        scratch_shapes=[
            dma((2, SEQS, 2)),
            dma((2, SEQS, 2)),
            dma((4, SEQS, 2)),
            dma((SEQS, 2)),
            dma((SEQS, 2)),
            dma((SEQS,)),
            dma((SEQS,)),
            dma((4, SEQS, 2)),
        ],
        compiler_params=pltpu.CompilerParams(collective_id=1, has_side_effects=True),
    )(own)


def mix_kernel(lengths, own, groups, out_w, columns, out):
    kv, tp = lax.axis_index("kv"), lax.axis_index("tp")
    live = lengths[sequence_of(pl.program_id(0), lengths)] > kv * SPAN

    @pl.when(live)
    def _():
        total = jnp.zeros((SPAN, SPAN), jnp.float32)
        own_w = out_w[:, pl.ds(pl.multiple_of(tp * SPAN, SPAN), SPAN)]
        for g in range(NTP):
            rows = jnp.where(tp == g, own[0], groups[g, 0])
            cols = jnp.where(tp == g, own_w, columns[g])
            part = jnp.dot(rows, cols, preferred_element_type=jnp.float32)
            total += part.astype(jnp.bfloat16).astype(jnp.float32)
        out[0] = total.astype(jnp.bfloat16)

    @pl.when(jnp.logical_not(live))
    def _():
        out[0] = jnp.zeros((SPAN, SPAN), jnp.bfloat16)


def mix(lengths, own, groups, out_weight, columns):
    once = dict(pipeline_mode=pl.Buffered(1))
    return pl.pallas_call(
        mix_kernel,
        name="mix",
        out_shape=jax.ShapeDtypeStruct((SEQS, SPAN, SPAN), jnp.bfloat16),
        grid_spec=pltpu.PrefetchScalarGridSpec(
            num_scalar_prefetch=1,
            grid=(SEQS,),
            in_specs=[
                pl.BlockSpec((1, SPAN, 2 * HD), lambda j, lens: (j, 0, 0)),
                pl.BlockSpec((NTP, 1, SPAN, 2 * HD), lambda j, lens: (0, j, 0, 0)),
                pl.BlockSpec((SPAN, MODEL), lambda j, lens: (0, 0), **once),
                pl.BlockSpec((NTP, SPAN, SPAN), lambda j, lens: (0, 0, 0), **once),
            ],
            out_specs=pl.BlockSpec((1, SPAN, SPAN), lambda j, lens: (sequence_of(j, lens), 0, 0)),
        ),
    )(lengths, own, groups, out_weight, columns)


def shards(inputs, query_weight, key_weight, value_weight, out_weight, chosen, lengths):
    queries, own = project(lengths, inputs, query_weight, key_weight, value_weight)
    cache, columns = spread(REACH, own, out_weight)
    attended = attend(lengths, chosen, queries, own, cache)
    groups = collect(REACH, attended)
    return mix(lengths, attended, groups, out_weight, columns)


def solution(mesh):
    placed = (
        P(None, "kv", None),
        P(None, "tp"),
        P(None, "tp"),
        P(None, "tp"),
        P("tp", None),
        P(None, "kv", None),
        P(),
    )
    return jax.shard_map(
        shards, mesh=mesh, in_specs=placed, out_specs=P(None, "kv", "tp"), check_vma=False
    )
```

```python
import jax
import jax.numpy as jnp
from jax import lax
from jax.experimental import pallas as pl
from jax.experimental.pallas import tpu as pltpu
from jax.sharding import PartitionSpec as P

HD = 128
KB = 64
TOPK = 32
SEQS = 4
SPAN = 256
MODEL = 2048
NZ, NX, NY = 8, 4, 4
NTP = 8
REACH = (7, 5, 3, 2)
NEAR_REACH = (7, 2, 1, 0)
LANES = 128
MORE = 8
COUNT = 124
REPEATS, LOCAL, LIVE, ORDER = 0, 1, 2, 3
CHUNK = 256
MESH = pl.DeviceIdType.MESH
ANY = pl.BlockSpec(memory_space=pl.ANY)
SMEM = pl.BlockSpec(memory_space=pltpu.SMEM)
VMEM = pl.BlockSpec(memory_space=pltpu.VMEM)


def sequence_of(slot, lengths):
    size = [lengths[b] for b in range(SEQS)]
    found = jnp.int32(0)
    for b in range(SEQS):
        rank = jnp.int32(0)
        for o in range(SEQS):
            if o < b:
                rank += (size[o] >= size[b]).astype(jnp.int32)
            elif o > b:
                rank += (size[o] > size[b]).astype(jnp.int32)
        found += jnp.where(rank == slot, b, 0)
    return found


def project_kernel(lengths, x, key_w, value_w, chosen, kv_out, plan, weights, named, packed):
    @pl.when(pl.program_id(0) == 0)
    def _():
        weights[:, :HD] = key_w[...]
        weights[:, HD:] = value_w[...]

    kv_out[0] = jnp.dot(x[0], weights[...], preferred_element_type=jnp.float32).astype(jnp.bfloat16)

    @pl.when(pl.program_id(0) == 0)
    def _():
        kv = lax.axis_index("kv")
        named[...] = jnp.full(named.shape, -1, jnp.int32)
        for b in range(SEQS):
            named[b * 4:(b + 1) * 4, :TOPK] = chosen[b]
        block = named[...]
        lane = lax.broadcasted_iota(jnp.int32, block.shape, 1)
        row = lax.broadcasted_iota(jnp.int32, block.shape, 0)
        i = row % 4
        length = jnp.full(block.shape, lengths[0])
        for b in range(1, SEQS):
            length = jnp.where(row // 4 == b, lengths[b], length)
        member = jnp.zeros(block.shape, jnp.int32)
        for e in range(TOPK):
            member |= (block[:, e:e + 1] == lane).astype(jnp.int32)
        member = jnp.where((kv * 4 + i) * KB < length, member, 0)
        repeats = jnp.sum((block == kv * 4 + i).astype(jnp.int32), axis=1, keepdims=True) - 1
        here = lane - kv * 4
        inside = (here >= 0) & (here < 4)
        local = jnp.sum(jnp.where(inside, member << jnp.where(inside, here, 0), 0), axis=1, keepdims=True)
        named[...] = jnp.where(here < 0, member << i, 0)
        live = jnp.int32(0)
        for b in range(SEQS):
            live += (lengths[b] > kv * SPAN).astype(jnp.int32)
        more = jnp.where(lane == REPEATS, repeats, jnp.where(lane == LOCAL, local, live))
        for j in range(SEQS):
            more = jnp.where(lane == ORDER + j, sequence_of(j, lengths), more)
        plan[MORE:, :] = more

        packed[...] = jnp.zeros(packed.shape, jnp.int32)
        for b in range(SEQS):
            packed[b:b + 1, :] = jnp.sum(named[b * 4:(b + 1) * 4, :], axis=0, keepdims=True)
        code = packed[...]
        lane = lax.broadcasted_iota(jnp.int32, code.shape, 1)
        held = (code != 0).astype(jnp.int32)
        code = lane + 256 * code
        steps = (1, 2, 4, 8, 16, 32, 64)
        upto = held
        for s in steps:
            upto += jnp.where(lane >= s, pltpu.roll(upto, s, 1), 0)
        count = jnp.sum(held, axis=1, keepdims=True)
        gap = lane - (upto - 1)
        for s in steps:
            there = pltpu.roll(code, LANES - s, 1)
            there_gap = pltpu.roll(gap, LANES - s, 1)
            take = (pltpu.roll(held, LANES - s, 1) != 0) & ((there_gap & s) != 0)
            stay = (held != 0) & ((gap & s) == 0)
            code = jnp.where(take, there, code)
            gap = jnp.where(take, there_gap, gap)
            held = (take | stay).astype(jnp.int32)
        plan[:MORE, :] = jnp.where(lane == COUNT, count, code)


def project(lengths, inputs, key_weight, value_weight, chosen):
    once = dict(pipeline_mode=pl.Buffered(1))
    rows = MORE + SEQS * (SPAN // KB)
    return pl.pallas_call(
        project_kernel,
        name="project",
        out_shape=(
            jax.ShapeDtypeStruct((SEQS, SPAN, 2 * HD), jnp.bfloat16),
            jax.ShapeDtypeStruct((rows, LANES), jnp.int32),
        ),
        grid_spec=pltpu.PrefetchScalarGridSpec(
            num_scalar_prefetch=1,
            grid=(SEQS,),
            in_specs=[
                pl.BlockSpec((1, SPAN, MODEL), lambda j, lens: (sequence_of(j, lens), 0, 0)),
                pl.BlockSpec((MODEL, HD), lambda j, lens: (0, 0), **once),
                pl.BlockSpec((MODEL, HD), lambda j, lens: (0, 0), **once),
                pl.BlockSpec((SEQS, SPAN // KB, TOPK), lambda j, lens: (0, 0, 0), **once),
            ],
            out_specs=(
                pl.BlockSpec((1, SPAN, 2 * HD), lambda j, lens: (j, 0, 0)),
                pl.BlockSpec((rows, LANES), lambda j, lens: (0, 0)),
            ),
            scratch_shapes=[
                pltpu.VMEM((MODEL, 2 * HD), jnp.bfloat16),
                pltpu.VMEM((rows - MORE, LANES), jnp.int32),
                pltpu.VMEM((MORE, LANES), jnp.int32),
            ],
        ),
    )(lengths, inputs, key_weight, value_weight, chosen)


def spread_kernel(reach, own, out_w, inputs, query_w, cache, columns, q_out, rows_in, weights,
                  load_sem, recv, up_sem, top_sem, relay_up, relay_down, right_sem, left_sem, pass_right, pass_left, w_send, w_recv):
    kv, tp = lax.axis_index("kv"), lax.axis_index("tp")
    z, x = kv // NX, kv % NX
    right = {"kv": z * NX + (x + 1) % NX}
    left = {"kv": z * NX + (x + NX - 1) % NX}
    x_right, x_left, x_far = (x + 1) % NX, (x + NX - 1) % NX, (x + 2) % NX
    half = SPAN // 2

    def load_rows(b):
        return pltpu.make_async_copy(inputs.at[b], rows_in.at[b], load_sem.at[b])

    load_w = pltpu.make_async_copy(query_w, weights, load_sem.at[SEQS])
    load_w.start()
    for b in range(SEQS):
        load_rows(b).start()

    above = {"kv": (z + 1) % NZ * NX + x}
    below = {"kv": (z + NZ - 1) % NZ * NX + x}
    top = {"kv": (NZ - 1) * NX + x}

    barrier = pltpu.get_barrier_semaphore()

    def greet(device):
        pl.semaphore_signal(barrier, inc=1, device_id=device, device_id_type=MESH)

    for d in (above, below, right, left):
        greet(d)
    for d in range(1, NTP):
        greet({"tp": (tp + d) % NTP})
    low = (z >= 1) & (z <= 2)

    @pl.when(low)
    def _():
        greet(top)

    @pl.when(z == NZ - 1)
    def _():
        for w in (1, 2):
            greet({"kv": w * NX + x})

    pl.semaphore_wait(barrier, 4 + NTP - 1 + low.astype(jnp.int32) + z // (NZ - 1) * 2)

    def piece(slot, owner_z, owner_x, h):
        first = pl.multiple_of((owner_z * NX + owner_x) * SPAN + h * half, half)
        return cache.at[slot, pl.ds(first, half)]

    def mine(slot, h):
        return own.at[slot, pl.ds(h * half, half)]

    def send(src, sem, slot, owner_z, owner_x, h, device):
        return pltpu.make_async_remote_copy(
            src_ref=src, dst_ref=piece(slot, owner_z, owner_x, h), send_sem=sem,
            recv_sem=recv.at[slot, owner_z * NX + owner_x, h],
            device_id=device, device_id_type=MESH)

    def arrived(slot, owner_z, owner_x, h):
        here = piece(slot, owner_z, owner_x, h)
        send(here, up_sem.at[slot, 0, h], slot, owner_z, owner_x, h, right).wait_recv()

    def start(copy):
        copy.start()

    def wait_send(copy):
        copy.wait_send()

    def goes_up(slot, d):
        climb = 3 if slot == 0 else NZ
        return (z + 1 <= reach[slot]) & (d <= climb)

    columns_of = (x, x_left, x_far, x_right)

    def whole(d):
        return (d == z) & ((z <= 2) | (z >= 5))

    def relay(c, h, src, act):
        @pl.when(z < (3 if c == 0 else 2))
        def _():
            act(send(src, relay_up.at[c, h], 0, 0, columns_of[c], h, above))

        @pl.when((z == 0) | (z >= 6))
        def _():
            act(send(src, relay_down.at[c, h], 0, 0, columns_of[c], h, below))

    def relay_piece(c, h, act):
        relay(c, h, piece(0, 0, columns_of[c], h), act)

    def along(slot, t, d, h, src, act):
        w = z - d
        plain = jnp.logical_not(whole(d)) if slot == 0 else z >= 0
        beside = plain | (z == 0)

        @pl.when(plain & goes_up(slot, d))
        def _():
            act(send(src, up_sem.at[slot, t, h], slot, w, x, h, above))

        if slot == 0:
            @pl.when(plain & (d >= 6))
            def _():
                act(send(src, up_sem.at[slot, t, h], slot, w, x, h, below))

            @pl.when(whole(d))
            def _():
                relay(0, h, src, act)

        @pl.when(beside)
        def _():
            act(send(src, right_sem.at[slot, t, h], slot, w, x, h, right))
            act(send(src, left_sem.at[slot, t, h], slot, w, x, h, left))

    def to_top(h):
        return send(mine(0, h), top_sem.at[h], 0, z, x, h, top)

    def each(body, slots=range(SEQS)):
        for slot in slots:
            @pl.when(z <= reach[slot])
            def _(slot=slot):
                body(slot)

    def distance(t):
        return t % 2 * ((t + 1) // 2) + (1 - t % 2) * ((NZ - t // 2) % NZ)

    def passing(slot, t, w, act):
        act(send(piece(slot, w, x_left, 0), pass_right.at[slot, t], slot, w, x_left, 0, right))
        act(send(piece(slot, w, x_right, 1), pass_left.at[slot, t], slot, w, x_right, 1, left))

    def around(t, slots=range(SEQS)):
        d = distance(t)
        w = z - d

        def body(slot):
            arrived(slot, w, x_left, 0)
            arrived(slot, w, x_right, 1)
            if slot == 0:
                @pl.when(jnp.logical_not(whole(d)) | (z == 0))
                def _():
                    passing(slot, t, w, start)

                @pl.when(whole(d))
                def _():
                    relay_piece(1, 0, start)
                    relay_piece(3, 1, start)
            else:
                passing(slot, t, w, start)

        each(body, slots)

    late = ((1, 1), (3, 0), (2, 0), (2, 1))

    def tail(t):
        @pl.when(whole(distance(t)) & (z <= reach[0]))
        def _():
            for c, h in late:
                arrived(0, 0, columns_of[c], h)
                relay_piece(c, h, start)

    def column(t):
        d = distance(t)

        def body(slot):
            for h in range(2):
                arrived(slot, z - d, x, h)
                along(slot, t, d, h, piece(slot, z - d, x, h), start)

        each(body)

    def finish(t):
        d = distance(t)
        w = z - d

        def rest(slot):
            for c, h in late:
                arrived(slot, w, columns_of[c], h)

        def body(slot):
            for h in range(2):
                along(slot, t, d, h, piece(slot, w, x, h), wait_send)
            if slot == 0:
                @pl.when(jnp.logical_not(whole(d)))
                def _():
                    rest(slot)

                @pl.when(jnp.logical_not(whole(d)) | (z == 0))
                def _():
                    passing(slot, t, w, wait_send)

                @pl.when(whole(d))
                def _():
                    for c, h in ((1, 0), (3, 1)) + late:
                        relay_piece(c, h, wait_send)
            else:
                rest(slot)
                passing(slot, t, w, wait_send)

        each(body)

    def column_copy(d):
        peer = (tp + d) % NTP
        first = pl.multiple_of(peer * SPAN, SPAN)
        return pltpu.make_async_remote_copy(
            src_ref=out_w.at[:, pl.ds(first, SPAN)], dst_ref=columns.at[tp],
            send_sem=w_send.at[d - 1], recv_sem=w_recv.at[d - 1],
            device_id={"tp": peer}, device_id_type=MESH)

    def begin(slot):
        for h in range(2):
            along(slot, 0, 0, h, mine(slot, h), start)

    @pl.when(low)
    def _():
        for h in range(2):
            to_top(h).start()

    each(begin, (0, 1))

    load_w.wait()
    for b in range(SEQS):
        load_rows(b).wait()
        q_out[b] = jnp.dot(rows_in[b], weights[...], preferred_element_type=jnp.float32).astype(jnp.bfloat16)

    around(0, (0,))
    each(begin, (2, 3))
    for d in range(1, NTP):
        column_copy(d).start()

    @pl.loop(1, NZ + 2)
    def _(t):
        @pl.when((t < NZ) & (distance(t) <= z))
        def _():
            column(t)

        @pl.when((t <= NZ) & (t > 1) & (distance(t - 1) <= z))
        def _():
            around(t - 1)

        @pl.when(t == 1)
        def _():
            around(0, (1, 2, 3))

        @pl.when(t >= 2)
        def _():
            tail(t - 2)

    @pl.loop(0, NZ)
    def _(t):
        @pl.when(distance(t) <= z)
        def _():
            finish(t)

    @pl.when(low)
    def _():
        for h in range(2):
            to_top(h).wait_send()

    for d in range(1, NTP):
        column_copy(d).wait()


def spread(reach, own, out_weight, inputs, query_weight):
    dma = pltpu.SemaphoreType.DMA
    return pl.pallas_call(
        lambda *refs: spread_kernel(reach, *refs),
        name="spread",
        out_shape=(
            jax.ShapeDtypeStruct((SEQS, NZ * NX * SPAN, 2 * HD), jnp.bfloat16),
            jax.ShapeDtypeStruct((NTP, SPAN, SPAN), jnp.bfloat16),
            jax.ShapeDtypeStruct((SEQS, SPAN, 2 * HD), jnp.bfloat16),
        ),
        in_specs=[ANY] * 4,
        out_specs=(ANY, ANY, VMEM),
        scratch_shapes=[
            pltpu.VMEM((SEQS, SPAN, MODEL), jnp.bfloat16),
            pltpu.VMEM((MODEL, 2 * HD), jnp.bfloat16),
            dma((SEQS + 1,)),
            dma((SEQS, NZ * NX, 2)),
            dma((SEQS, NZ, 2)),
            dma((2,)),
            dma((NX, 2)),
            dma((NX, 2)),
            dma((SEQS, NZ, 2)),
            dma((SEQS, NZ, 2)),
            dma((SEQS, NZ)),
            dma((SEQS, NZ)),
            dma((NTP - 1,)),
            dma((NTP - 1,)),
        ],
        compiler_params=pltpu.CompilerParams(
            collective_id=0 if reach == REACH else 1, has_side_effects=True
        ),
    )(own, out_weight, inputs, query_weight)


def attend_kernel(lengths, plan, q, own, cache, out, keys, scores, high, total, acc, own_sems, sems):
    kv = lax.axis_index("kv")
    slots = plan[MORE, LIVE]
    blocks = SPAN // KB
    heads = 2

    def sequence(slot):
        b = plan[MORE, ORDER + slot]
        return b, plan[b, COUNT]

    def own_copy(slot):
        return pltpu.make_async_copy(own.at[slot], keys.at[slot % 2, pl.ds(0, SPAN)], own_sems.at[slot % 2])

    def block_copy(slot, block, e):
        row = pl.multiple_of(block * KB, KB)
        to = pl.multiple_of(SPAN + e * KB, KB)
        return pltpu.make_async_copy(
            cache.at[slot, pl.ds(row, KB)], keys.at[slot % 2, pl.ds(to, KB)], sems.at[slot % 2])

    def fetch(slot):
        b, n = sequence(slot)
        own_copy(slot).start()

        @pl.loop(0, n)
        def _(e):
            block_copy(slot, plan[b, e] % 256, e).start()

        past = pl.ds(pl.multiple_of(SPAN + n * KB, KB), 3 * KB)
        keys[slot % 2, past, :] = jnp.zeros((3 * KB, 2 * HD), jnp.bfloat16)

    def part(h, i):
        return slice(h * SPAN + i * KB, h * SPAN + (i + 1) * KB)

    def compute(slot):
        b, n = sequence(slot)
        held = keys.at[slot % 2]
        chunks = 1 + (n + 3) // 4
        own_copy(slot).wait()
        both = q[b]
        stacked = jnp.concatenate([both[:, :HD], both[:, HD:]], axis=0)
        lane = lax.broadcasted_iota(jnp.int32, (1, CHUNK), 1)
        place = lane // KB

        def score(first):
            return lax.dot_general(stacked, held[pl.ds(first, CHUNK), :HD], (((1,), (1,)), ((), ())),
                                   preferred_element_type=jnp.float32) * (HD ** -0.5)

        s = score(0)
        col = lax.broadcasted_iota(jnp.int32, (KB, CHUNK), 1)
        row = lax.broadcasted_iota(jnp.int32, (KB, CHUNK), 0)
        for i in range(blocks):
            bits = plan[MORE + b * 4 + i, LOCAL] | (1 << i)
            named = jnp.zeros((1, CHUNK), jnp.int32)
            for p in range(blocks):
                named = jnp.where(place == p, (bits >> p) & 1, named)
            limit = jnp.where(named != 0, lane, SPAN)
            for h in range(heads):
                now = jnp.where(limit <= row + i * KB, s[part(h, i)], -jnp.inf)
                scores[0, part(h, i), :] = now
                high[part(h, i), :] = jnp.maximum(now[:, :HD], now[:, HD:])

        @pl.loop(0, n)
        def _(e):
            block_copy(slot, 0, e).wait()

        @pl.loop(1, chunks)
        def _(c):
            s = score(pl.multiple_of(c * CHUNK, CHUNK))
            codes = []
            for p in range(blocks):
                e = (c - 1) * 4 + p
                codes.append(jnp.where(e < n, plan[b, e] // 256, 0))
            for i in range(blocks):
                shift = jnp.zeros((1, CHUNK), jnp.float32)
                for p in range(blocks):
                    absent = jnp.where((codes[p] >> i) & 1 != 0, jnp.float32(0), -jnp.inf)
                    shift = jnp.where(place == p, absent, shift)
                for h in range(heads):
                    now = s[part(h, i)] + shift
                    scores[c, part(h, i), :] = now
                    high[part(h, i), :] = jnp.maximum(high[part(h, i), :], jnp.maximum(now[:, :HD], now[:, HD:]))

        for h in range(heads):
            for i in range(blocks):
                top = jnp.max(high[part(h, i), :], axis=1, keepdims=True)
                high[part(h, i), :] = jnp.broadcast_to(top, (KB, HD))
        total[...] = jnp.zeros_like(total)

        @pl.loop(0, chunks)
        def _(c):
            for h in range(heads):
                for i in range(blocks):
                    top = high[part(h, i), :]
                    left = jnp.exp(scores[c, part(h, i), :HD] - top)
                    right = jnp.exp(scores[c, part(h, i), HD:] - top)
                    scores[c, part(h, i), :HD] = left
                    scores[c, part(h, i), HD:] = right
                    total[part(h, i), :] += left + right

        again = jnp.int32(0)
        for i in range(blocks):
            again += plan[MORE + b * 4 + i, REPEATS]

        def self_part(h, i):
            return jnp.where(col == row + i * KB, scores[0, part(h, i), :], 0.0)

        @pl.when(again > 0)
        def _():
            for h in range(heads):
                for i in range(blocks):
                    e = self_part(h, i)
                    times = plan[MORE + b * 4 + i, REPEATS].astype(jnp.float32)
                    total[part(h, i), :] += times * (e[:, :HD] + e[:, HD:])

        for h in range(heads):
            for i in range(blocks):
                share = 1.0 / jnp.sum(total[part(h, i), :], axis=1, keepdims=True)
                total[part(h, i), :] = jnp.broadcast_to(share, (KB, HD))
        acc[...] = jnp.zeros_like(acc)

        @pl.when(again > 0)
        def _():
            for h in range(heads):
                for i in range(blocks):
                    share = total[part(h, i), :]
                    e = self_part(h, i)
                    weight = jnp.concatenate([e[:, :HD] * share, e[:, HD:] * share], axis=1)
                    times = plan[MORE + b * 4 + i, REPEATS].astype(jnp.float32)
                    acc[part(h, i), :] = times * jnp.dot(
                        weight.astype(jnp.bfloat16), held[:SPAN, HD:], preferred_element_type=jnp.float32)

        @pl.loop(0, chunks)
        def _(c):
            share = total[...]
            weight = jnp.concatenate([scores[c, :, :HD] * share, scores[c, :, HD:] * share], axis=1)
            acc[...] += jnp.dot(weight.astype(jnp.bfloat16),
                                held[pl.ds(pl.multiple_of(c * CHUNK, CHUNK), CHUNK), HD:],
                                preferred_element_type=jnp.float32)

        pos = kv * SPAN + lax.broadcasted_iota(jnp.int32, (SPAN, HD), 0)
        for h in range(heads):
            done = jnp.where(pos < lengths[b], acc[h * SPAN:(h + 1) * SPAN, :], 0.0)
            out[slot, :, h * HD:(h + 1) * HD] = done.astype(jnp.bfloat16)

    @pl.when(slots > 0)
    def _():
        fetch(jnp.int32(0))

    @pl.loop(0, slots)
    def _(slot):
        @pl.when(slot + 1 < slots)
        def _():
            fetch(slot + 1)

        compute(slot)


def attend(lengths, plan, q, own, cache):
    most = NZ * NX * (SPAN // KB)
    rows = 2 * SPAN
    return pl.pallas_call(
        attend_kernel,
        name="attend",
        out_shape=jax.ShapeDtypeStruct((SEQS, SPAN, 2 * HD), jnp.bfloat16),
        in_specs=[SMEM, SMEM, VMEM, ANY, ANY],
        out_specs=VMEM,
        scratch_shapes=[
            pltpu.VMEM((2, SPAN + most * KB, 2 * HD), jnp.bfloat16),
            pltpu.VMEM((1 + most // 4, rows, CHUNK), jnp.float32),
            pltpu.VMEM((rows, HD), jnp.float32),
            pltpu.VMEM((rows, HD), jnp.float32),
            pltpu.VMEM((rows, HD), jnp.float32),
            pltpu.SemaphoreType.DMA((2,)),
            pltpu.SemaphoreType.DMA((2,)),
        ],
    )(lengths, plan, q, own, cache)


def collect_kernel(reach, own, groups, next_recv, prev_recv, core_recv, next_send, prev_send,
                   next_pass, prev_pass, core_send):
    kv, tp = lax.axis_index("kv"), lax.axis_index("tp")
    z = kv // NX
    y, core = tp // 2, tp % 2
    y_next, y_prev, y_far = (y + 1) % NY, (y + NY - 1) % NY, (y + 2) % NY
    after, before = {"tp": y_next * 2 + core}, {"tp": y_prev * 2 + core}
    partner = {"tp": y * 2 + 1 - core}
    half = SPAN // 2

    barrier = pltpu.get_barrier_semaphore()
    for d in (after, before, partner):
        pl.semaphore_signal(barrier, inc=1, device_id=d, device_id_type=MESH)
    pl.semaphore_wait(barrier, 3)

    def piece(owner_y, owner_core, slot, h):
        return groups.at[owner_y * 2 + owner_core, slot, pl.ds(h * half, half)]

    def copy(src, dst, send_sem, recv_sem, device):
        return pltpu.make_async_remote_copy(
            src_ref=src, dst_ref=dst, send_sem=send_sem, recv_sem=recv_sem,
            device_id=device, device_id_type=MESH)

    def mine(slot, h):
        return own.at[slot, pl.ds(h * half, half)]

    def to_next(slot, h):
        return copy(mine(slot, h), piece(y, core, slot, h), next_send.at[slot, h],
                    next_recv.at[0, slot, h], after)

    def to_prev(slot, h):
        return copy(mine(slot, h), piece(y, core, slot, h), prev_send.at[slot, h],
                    prev_recv.at[0, slot, h], before)

    def on_next(slot):
        here = piece(y_prev, core, slot, 0)
        return copy(here, here, next_pass.at[slot], next_recv.at[1, slot, 0], after)

    def on_prev(slot):
        here = piece(y_next, core, slot, 1)
        return copy(here, here, prev_pass.at[slot], prev_recv.at[1, slot, 1], before)

    def across(far, owner_y, slot, h, src=None):
        here = piece(owner_y, core, slot, h)
        return copy(here if src is None else src, here, core_send.at[far, slot, h],
                    core_recv.at[far, slot, h], partner)

    def each(body):
        for slot in range(SEQS):
            @pl.when(z <= reach[slot])
            def _(slot=slot):
                body(slot)

    def begin(slot):
        to_next(slot, 0).start()
        to_prev(slot, 1).start()
        to_next(slot, 1).start()
        to_prev(slot, 0).start()
        for h in range(2):
            across(0, y, slot, h, mine(slot, h)).start()

    def relay(slot):
        to_next(slot, 0).wait_recv()
        on_next(slot).start()
        across(1, y_prev, slot, 0).start()
        to_prev(slot, 1).wait_recv()
        on_prev(slot).start()
        across(2, y_next, slot, 1).start()
        to_next(slot, 1).wait_recv()
        across(1, y_prev, slot, 1).start()
        to_prev(slot, 0).wait_recv()
        across(2, y_next, slot, 0).start()

    def far(slot):
        on_next(slot).wait_recv()
        across(3, y_far, slot, 0).start()
        on_prev(slot).wait_recv()
        across(3, y_far, slot, 1).start()

    def finish(slot):
        for h in range(2):
            to_next(slot, h).wait_send()
            to_prev(slot, h).wait_send()
            across(0, y, slot, h).wait()
            across(1, y_prev, slot, h).wait()
            across(2, y_next, slot, h).wait()
            across(3, y_far, slot, h).wait()
        on_next(slot).wait_send()
        on_prev(slot).wait_send()

    each(begin)
    each(relay)
    each(far)
    each(finish)


def collect(reach, own):
    dma = pltpu.SemaphoreType.DMA
    return pl.pallas_call(
        lambda *refs: collect_kernel(reach, *refs),
        name="collect",
        out_shape=jax.ShapeDtypeStruct((NTP, SEQS, SPAN, 2 * HD), jnp.bfloat16),
        in_specs=[ANY],
        out_specs=ANY,
        scratch_shapes=[
            dma((2, SEQS, 2)),
            dma((2, SEQS, 2)),
            dma((4, SEQS, 2)),
            dma((SEQS, 2)),
            dma((SEQS, 2)),
            dma((SEQS,)),
            dma((SEQS,)),
            dma((4, SEQS, 2)),
        ],
        compiler_params=pltpu.CompilerParams(collective_id=2 if reach == REACH else 3, has_side_effects=True),
    )(own)


def mix_kernel(plan, own, groups, out_w, columns, out):
    tp = lax.axis_index("tp")
    live = pl.program_id(0) < plan[MORE, LIVE]

    @pl.when(live)
    def _():
        total = jnp.zeros((SPAN, SPAN), jnp.float32)
        own_w = out_w[:, pl.ds(pl.multiple_of(tp * SPAN, SPAN), SPAN)]
        for g in range(NTP):
            rows = jnp.where(tp == g, own[0], groups[g, 0])
            cols = jnp.where(tp == g, own_w, columns[g])
            part = jnp.dot(rows, cols, preferred_element_type=jnp.float32)
            total += part.astype(jnp.bfloat16).astype(jnp.float32)
        out[0] = total.astype(jnp.bfloat16)

    @pl.when(jnp.logical_not(live))
    def _():
        out[0] = jnp.zeros((SPAN, SPAN), jnp.bfloat16)


def mix(plan, own, groups, out_weight, columns):
    once = dict(pipeline_mode=pl.Buffered(1))

    def slot(j, plan):
        return jnp.minimum(j, jnp.maximum(plan[MORE, LIVE] - 1, 0))

    return pl.pallas_call(
        mix_kernel,
        name="mix",
        out_shape=jax.ShapeDtypeStruct((SEQS, SPAN, SPAN), jnp.bfloat16),
        grid_spec=pltpu.PrefetchScalarGridSpec(
            num_scalar_prefetch=1,
            grid=(SEQS,),
            in_specs=[
                pl.BlockSpec((1, SPAN, 2 * HD), lambda j, plan: (slot(j, plan), 0, 0)),
                pl.BlockSpec((NTP, 1, SPAN, 2 * HD), lambda j, plan: (0, slot(j, plan), 0, 0)),
                pl.BlockSpec((SPAN, MODEL), lambda j, plan: (0, 0), **once),
                pl.BlockSpec((NTP, SPAN, SPAN), lambda j, plan: (0, 0, 0), **once),
            ],
            out_specs=pl.BlockSpec((1, SPAN, SPAN), lambda j, plan: (plan[MORE, ORDER + j], 0, 0)),
        ),
    )(plan, own, groups, out_weight, columns)


def shards(inputs, query_weight, key_weight, value_weight, out_weight, chosen, lengths):
    own, plan = project(lengths, inputs, key_weight, value_weight, chosen)

    def rest(reach):
        cache, columns, queries = spread(reach, own, out_weight, inputs, query_weight)
        attended = attend(lengths, plan, queries, own, cache)
        groups = collect(reach, attended)
        return mix(plan, attended, groups, out_weight, columns)

    near = jnp.bool_(True)
    for j in range(1, SEQS):
        longer = jnp.sum((lengths > (NEAR_REACH[j] + 1) * NX * SPAN).astype(jnp.int32))
        near &= longer <= j
    return lax.cond(near, lambda: rest(NEAR_REACH), lambda: rest(REACH))


def solution(mesh):
    placed = (
        P(None, "kv", None),
        P(None, "tp"),
        P(None, "tp"),
        P(None, "tp"),
        P("tp", None),
        P(None, "kv", None),
        P(),
    )
    return jax.shard_map(
        shards, mesh=mesh, in_specs=placed, out_specs=P(None, "kv", "tp"), check_vma=False
    )
```

```python
import jax
import jax.numpy as jnp
from jax import lax
from jax.experimental import pallas as pl
from jax.experimental.pallas import tpu as pltpu
from jax.sharding import PartitionSpec as P

HD = 128
KB = 64
TOPK = 32
SEQS = 4
SPAN = 256
MODEL = 2048
NZ, NX, NY = 8, 4, 4
NTP = 8
REACH = (7, 5, 3, 2)
NEAR_REACH = (7, 2, 1, 0)
LANES = 128
MORE = 8
COUNT = 124
REPEATS, LOCAL, LIVE, ORDER = 0, 1, 2, 3
CHUNK = 256
MESH = pl.DeviceIdType.MESH
ANY = pl.BlockSpec(memory_space=pl.ANY)
SMEM = pl.BlockSpec(memory_space=pltpu.SMEM)
VMEM = pl.BlockSpec(memory_space=pltpu.VMEM)


def sequence_of(slot, lengths):
    size = [lengths[b] for b in range(SEQS)]
    found = jnp.int32(0)
    for b in range(SEQS):
        rank = jnp.int32(0)
        for o in range(SEQS):
            if o < b:
                rank += (size[o] >= size[b]).astype(jnp.int32)
            elif o > b:
                rank += (size[o] > size[b]).astype(jnp.int32)
        found += jnp.where(rank == slot, b, 0)
    return found


def make_plan(kv, lengths, chosen, plan, named, packed):
    named[...] = jnp.full(named.shape, -1, jnp.int32)
    for b in range(SEQS):
        named[b * 4:(b + 1) * 4, :TOPK] = chosen[b]
    block = named[...]
    lane = lax.broadcasted_iota(jnp.int32, block.shape, 1)
    row = lax.broadcasted_iota(jnp.int32, block.shape, 0)
    i = row % 4
    length = jnp.full(block.shape, lengths[0])
    for b in range(1, SEQS):
        length = jnp.where(row // 4 == b, lengths[b], length)
    member = jnp.zeros(block.shape, jnp.int32)
    for e in range(TOPK):
        member |= (block[:, e:e + 1] == lane).astype(jnp.int32)
    member = jnp.where((kv * 4 + i) * KB < length, member, 0)
    repeats = jnp.sum((block == kv * 4 + i).astype(jnp.int32), axis=1, keepdims=True) - 1
    here = lane - kv * 4
    inside = (here >= 0) & (here < 4)
    local = jnp.sum(jnp.where(inside, member << jnp.where(inside, here, 0), 0), axis=1, keepdims=True)
    named[...] = jnp.where(here < 0, member << i, 0)
    live = jnp.int32(0)
    for b in range(SEQS):
        live += (lengths[b] > kv * SPAN).astype(jnp.int32)
    more = jnp.where(lane == REPEATS, repeats, jnp.where(lane == LOCAL, local, live))
    for j in range(SEQS):
        more = jnp.where(lane == ORDER + j, sequence_of(j, lengths), more)
    plan[MORE:, :] = more

    packed[...] = jnp.zeros(packed.shape, jnp.int32)
    for b in range(SEQS):
        packed[b:b + 1, :] = jnp.sum(named[b * 4:(b + 1) * 4, :], axis=0, keepdims=True)
    code = packed[...]
    lane = lax.broadcasted_iota(jnp.int32, code.shape, 1)
    held = (code != 0).astype(jnp.int32)
    code = lane + 256 * code
    steps = (1, 2, 4, 8, 16, 32, 64)
    upto = held
    for s in steps:
        upto += jnp.where(lane >= s, pltpu.roll(upto, s, 1), 0)
    count = jnp.sum(held, axis=1, keepdims=True)
    gap = lane - (upto - 1)
    for s in steps:
        there = pltpu.roll(code, LANES - s, 1)
        there_gap = pltpu.roll(gap, LANES - s, 1)
        take = (pltpu.roll(held, LANES - s, 1) != 0) & ((there_gap & s) != 0)
        stay = (held != 0) & ((gap & s) == 0)
        code = jnp.where(take, there, code)
        gap = jnp.where(take, there_gap, gap)
        held = (take | stay).astype(jnp.int32)
    plan[:MORE, :] = jnp.where(lane == COUNT, count, code)


def spread_kernel(reach, lengths, chosen, inputs, query_w, key_w, value_w, out_w,
                  cache, columns, q_out, plan, held, rows_in, q_weights, kv_weights, projected,
                  named, packed, load_sem, store_sem, recv, up_sem, beside_sem, once_sem):
    kv, tp = lax.axis_index("kv"), lax.axis_index("tp")
    z, x = kv // NX, kv % NX
    right = {"kv": z * NX + (x + 1) % NX}
    left = {"kv": z * NX + (x + NX - 1) % NX}
    x_right, x_left, x_far = (x + 1) % NX, (x + NX - 1) % NX, (x + 2) % NX
    half = SPAN // 2
    TO_TOP, RELAY_UP, RELAY_DOWN, W_SEND, W_RECV = range(5)
    COLUMN, LEFT, RIGHT, LATE = 0, 2, 3, 4

    loads = [
        pltpu.make_async_copy(key_w, kv_weights.at[:, pl.ds(0, HD)], load_sem.at[0]),
        pltpu.make_async_copy(value_w, kv_weights.at[:, pl.ds(HD, HD)], load_sem.at[1]),
    ]
    loads += [pltpu.make_async_copy(inputs.at[b], rows_in.at[b], load_sem.at[2 + b]) for b in range(SEQS)]
    load_q = pltpu.make_async_copy(query_w, q_weights, load_sem.at[2 + SEQS])
    for load in loads:
        load.start()
    load_q.start()

    above = {"kv": (z + 1) % NZ * NX + x}
    below = {"kv": (z + NZ - 1) % NZ * NX + x}
    top = {"kv": (NZ - 1) * NX + x}

    barrier = pltpu.get_barrier_semaphore()

    def greet(device):
        pl.semaphore_signal(barrier, inc=1, device_id=device, device_id_type=MESH)

    for d in (above, below, right, left):
        greet(d)
    for d in range(1, NTP):
        greet({"tp": (tp + d) % NTP})
    low = (z >= 1) & (z <= 2)

    @pl.when(low)
    def _():
        greet(top)

    @pl.when(z == NZ - 1)
    def _():
        for w in (1, 2):
            greet({"kv": w * NX + x})

    loads[0].wait()
    loads[1].wait()
    for b in range(SEQS):
        loads[2 + b].wait()
        projected[b] = jnp.dot(rows_in[b], kv_weights[...], preferred_element_type=jnp.float32).astype(jnp.bfloat16)
    for slot in range(SEQS):
        held[slot, pl.ds(pl.multiple_of(kv * SPAN, SPAN), SPAN), :] = projected[sequence_of(slot, lengths)]

    pl.semaphore_wait(barrier, 4 + NTP - 1 + low.astype(jnp.int32) + z // (NZ - 1) * 2)

    def piece(slot, owner_z, owner_x, h):
        first = pl.multiple_of((owner_z * NX + owner_x) * SPAN + h * half, half)
        return held.at[slot, pl.ds(first, half)]

    def mine(slot, h):
        return piece(slot, z, x, h)

    def store(slot, w):
        span = pl.ds(pl.multiple_of(w * NX * SPAN, NX * SPAN), NX * SPAN)
        return pltpu.make_async_copy(held.at[slot, span], cache.at[slot, span], store_sem.at[row(slot, w)])

    def row(slot, w):
        return sum(reach[o] + 1 for o in range(slot)) + w

    def send(src, sem, slot, owner_z, owner_x, h, kind, device):
        return pltpu.make_async_remote_copy(
            src_ref=src, dst_ref=piece(slot, owner_z, owner_x, h), send_sem=sem,
            recv_sem=recv.at[row(slot, owner_z), kind],
            device_id=device, device_id_type=MESH)

    def arrived(slot, w, kind):
        size = SPAN * 2 if kind == LATE else half
        there = held.at[slot, pl.ds(0, size)]
        pltpu.make_async_remote_copy(
            src_ref=there, dst_ref=there, send_sem=up_sem.at[row(slot, w)],
            recv_sem=recv.at[row(slot, w), kind], device_id=right, device_id_type=MESH).wait_recv()

    def sent(slot, sem, pieces):
        there = held.at[slot, pl.ds(0, pieces * half)]
        pltpu.make_async_remote_copy(
            src_ref=there, dst_ref=there, send_sem=sem, recv_sem=recv.at[0, 0],
            device_id=right, device_id_type=MESH).wait_send()

    def goes_up(slot, d):
        climb = 3 if slot == 0 else NZ
        return (z + 1 <= reach[slot]) & (d <= climb)

    columns_of = (x, x_left, x_far, x_right)

    def whole(d):
        return (d == z) & ((z <= 2) | (z >= 5))

    def relay(c, h, kind):
        src = piece(0, 0, columns_of[c], h)

        @pl.when(z < (3 if c == 0 else 2))
        def _():
            send(src, once_sem.at[RELAY_UP], 0, 0, columns_of[c], h, kind, above).start()

        @pl.when((z == 0) | (z >= 6))
        def _():
            send(src, once_sem.at[RELAY_DOWN], 0, 0, columns_of[c], h, kind, below).start()

    def plain(slot, d):
        return jnp.logical_not(whole(d)) if slot == 0 else z >= 0

    def onward(slot, d):
        up = plain(slot, d) & goes_up(slot, d)
        down = plain(slot, d) & (d >= 6) if slot == 0 else z < 0
        return up, down

    def along(slot, d, h):
        w = z - d
        src = piece(slot, w, x, h)
        up, down = onward(slot, d)

        @pl.when(up)
        def _():
            send(src, up_sem.at[row(slot, w)], slot, w, x, h, COLUMN + h, above).start()

        if slot == 0:
            @pl.when(down)
            def _():
                send(src, up_sem.at[row(slot, w)], slot, w, x, h, COLUMN + h, below).start()

            @pl.when(whole(d))
            def _():
                relay(0, h, COLUMN + h)

        @pl.when(plain(slot, d) | (z == 0))
        def _():
            sem = beside_sem.at[row(slot, w)]
            send(src, sem, slot, w, x, h, LEFT if h == 0 else LATE, right).start()
            send(src, sem, slot, w, x, h, LATE if h == 0 else RIGHT, left).start()

    def to_top(h):
        return send(mine(0, h), once_sem.at[TO_TOP], 0, z, x, h, COLUMN + h, top)

    def each(body, slots=range(SEQS)):
        for slot in slots:
            @pl.when(z <= reach[slot])
            def _(slot=slot):
                body(slot)

    def distance(t):
        return t % 2 * ((t + 1) // 2) + (1 - t % 2) * ((NZ - t // 2) % NZ)

    def around(t, slots=range(SEQS)):
        d = distance(t)
        w = z - d

        def passing(slot):
            sem = beside_sem.at[row(slot, w)]
            send(piece(slot, w, x_left, 0), sem, slot, w, x_left, 0, LATE, right).start()
            send(piece(slot, w, x_right, 1), sem, slot, w, x_right, 1, LATE, left).start()

        def body(slot):
            arrived(slot, w, LEFT)
            arrived(slot, w, RIGHT)
            if slot == 0:
                @pl.when(plain(slot, d) | (z == 0))
                def _():
                    passing(slot)

                @pl.when(whole(d))
                def _():
                    relay(1, 0, LEFT)
                    relay(3, 1, RIGHT)
            else:
                passing(slot)

        each(body, slots)

    def tail(t):
        @pl.when(whole(distance(t)) & (z <= reach[0]))
        def _():
            arrived(0, 0, LATE)
            for c, h in ((1, 1), (3, 0), (2, 0), (2, 1)):
                relay(c, h, LATE)

    def column(t):
        d = distance(t)

        def body(slot):
            for h in range(2):
                arrived(slot, z - d, COLUMN + h)
                along(slot, d, h)

        each(body)

    def settle(t):
        d = distance(t)
        w = z - d

        def body(slot):
            if slot == 0:
                @pl.when(plain(slot, d))
                def _():
                    arrived(slot, w, LATE)
            else:
                arrived(slot, w, LATE)
            store(slot, w).start()

        each(body)

    def finish(t):
        d = distance(t)
        w = z - d

        def body(slot):
            up, down = onward(slot, d)

            @pl.when(up | down)
            def _():
                sent(slot, up_sem.at[row(slot, w)], 2)

            @pl.when(plain(slot, d) | (z == 0))
            def _():
                sent(slot, beside_sem.at[row(slot, w)], 6)

            store(slot, w).wait()

        each(body)

    def column_copy(d):
        peer = (tp + d) % NTP
        first = pl.multiple_of(peer * SPAN, SPAN)
        return pltpu.make_async_remote_copy(
            src_ref=out_w.at[:, pl.ds(first, SPAN)], dst_ref=columns.at[tp],
            send_sem=once_sem.at[W_SEND], recv_sem=once_sem.at[W_RECV],
            device_id={"tp": peer}, device_id_type=MESH)

    def begin(slot):
        for h in range(2):
            along(slot, 0, h)

    @pl.when(low)
    def _():
        for h in range(2):
            to_top(h).start()

    each(begin, (0, 1))

    load_q.wait()
    for b in range(SEQS):
        q_out[b] = jnp.dot(rows_in[b], q_weights[...], preferred_element_type=jnp.float32).astype(jnp.bfloat16)
    make_plan(kv, lengths, chosen, plan, named, packed)

    around(0, (0,))
    each(begin, (2, 3))
    for d in range(1, NTP):
        column_copy(d).start()

    @pl.loop(1, NZ + 4)
    def _(t):
        @pl.when((t < NZ) & (distance(t) <= z))
        def _():
            column(t)

        @pl.when((t - 3 < NZ) & (t - 3 > 0) & (distance(jnp.maximum(t - 3, 0)) <= z))
        def _():
            around(t - 3)

        @pl.when(t == 1)
        def _():
            around(0, (1, 2, 3))

        @pl.when((t - 4 >= 0) & (t - 4 < NZ))
        def _():
            tail(jnp.maximum(t - 4, 0))

    @pl.loop(0, NZ)
    def _(t):
        @pl.when(distance(t) <= z)
        def _():
            settle(t)

    @pl.loop(0, NZ)
    def _(t):
        @pl.when(distance(t) <= z)
        def _():
            finish(t)

    @pl.when(low)
    def _():
        sent(0, once_sem.at[TO_TOP], 2)

    climbs = z <= reach[0]

    @pl.when(climbs & (z < 2))
    def _():
        sent(0, once_sem.at[RELAY_UP], 8)

    @pl.when(climbs & (z == 2))
    def _():
        sent(0, once_sem.at[RELAY_UP], 2)

    @pl.when(climbs & ((z == 0) | (z >= 6)))
    def _():
        sent(0, once_sem.at[RELAY_DOWN], 8)

    others = columns.at[pl.ds(0, NTP - 1)]
    pltpu.make_async_remote_copy(
        src_ref=others, dst_ref=others, send_sem=once_sem.at[W_SEND], recv_sem=once_sem.at[W_RECV],
        device_id=right, device_id_type=MESH).wait()


def spread(reach, lengths, chosen, inputs, query_weight, key_weight, value_weight, out_weight):
    dma = pltpu.SemaphoreType.DMA
    named = SEQS * (SPAN // KB)
    rows = sum(r + 1 for r in reach)
    return pl.pallas_call(
        lambda *refs: spread_kernel(reach, *refs),
        name="spread",
        out_shape=(
            jax.ShapeDtypeStruct((SEQS, NZ * NX * SPAN, 2 * HD), jnp.bfloat16),
            jax.ShapeDtypeStruct((NTP, SPAN, SPAN), jnp.bfloat16),
            jax.ShapeDtypeStruct((SEQS, SPAN, 2 * HD), jnp.bfloat16),
            jax.ShapeDtypeStruct((MORE + named, LANES), jnp.int32),
        ),
        in_specs=[SMEM, VMEM] + [ANY] * 5,
        out_specs=(ANY, ANY, VMEM, VMEM),
        scratch_shapes=[
            pltpu.VMEM((SEQS, NZ * NX * SPAN, 2 * HD), jnp.bfloat16),
            pltpu.VMEM((SEQS, SPAN, MODEL), jnp.bfloat16),
            pltpu.VMEM((MODEL, 2 * HD), jnp.bfloat16),
            pltpu.VMEM((MODEL, 2 * HD), jnp.bfloat16),
            pltpu.VMEM((SEQS, SPAN, 2 * HD), jnp.bfloat16),
            pltpu.VMEM((named, LANES), jnp.int32),
            pltpu.VMEM((MORE, LANES), jnp.int32),
            dma((SEQS + 3,)),
            dma((rows,)),
            dma((rows, 5)),
            dma((rows,)),
            dma((rows,)),
            dma((5,)),
        ],
        compiler_params=pltpu.CompilerParams(
            collective_id=0 if reach == REACH else 1, has_side_effects=True
        ),
    )(lengths, chosen, inputs, query_weight, key_weight, value_weight, out_weight)


def attend_kernel(lengths, plan, q, cache, out, keys, scores, high, total, acc, own_sems, sems):
    kv = lax.axis_index("kv")
    slots = plan[MORE, LIVE]
    blocks = SPAN // KB
    heads = 2

    def sequence(slot):
        b = plan[MORE, ORDER + slot]
        return b, plan[b, COUNT]

    def own_copy(slot):
        span = pl.ds(pl.multiple_of(kv * SPAN, SPAN), SPAN)
        return pltpu.make_async_copy(
            cache.at[slot, span], keys.at[slot % 2, pl.ds(0, SPAN)], own_sems.at[slot % 2])

    def block_copy(slot, block, e):
        row = pl.multiple_of(block * KB, KB)
        to = pl.multiple_of(SPAN + e * KB, KB)
        return pltpu.make_async_copy(
            cache.at[slot, pl.ds(row, KB)], keys.at[slot % 2, pl.ds(to, KB)], sems.at[slot % 2])

    def fetch(slot):
        b, n = sequence(slot)
        own_copy(slot).start()

        @pl.loop(0, n)
        def _(e):
            block_copy(slot, plan[b, e] % 256, e).start()

        past = pl.ds(pl.multiple_of(SPAN + n * KB, KB), 3 * KB)
        keys[slot % 2, past, :] = jnp.zeros((3 * KB, 2 * HD), jnp.bfloat16)

    def part(h, i):
        return slice(h * SPAN + i * KB, h * SPAN + (i + 1) * KB)

    def compute(slot):
        b, n = sequence(slot)
        held = keys.at[slot % 2]
        chunks = 1 + (n + 3) // 4
        own_copy(slot).wait()
        both = q[b]
        stacked = jnp.concatenate([both[:, :HD], both[:, HD:]], axis=0)
        lane = lax.broadcasted_iota(jnp.int32, (1, CHUNK), 1)
        place = lane // KB

        def score(first):
            return lax.dot_general(stacked, held[pl.ds(first, CHUNK), :HD], (((1,), (1,)), ((), ())),
                                   preferred_element_type=jnp.float32) * (HD ** -0.5)

        s = score(0)
        col = lax.broadcasted_iota(jnp.int32, (KB, CHUNK), 1)
        row = lax.broadcasted_iota(jnp.int32, (KB, CHUNK), 0)
        for i in range(blocks):
            bits = plan[MORE + b * 4 + i, LOCAL] | (1 << i)
            named = jnp.zeros((1, CHUNK), jnp.int32)
            for p in range(blocks):
                named = jnp.where(place == p, (bits >> p) & 1, named)
            limit = jnp.where(named != 0, lane, SPAN)
            for h in range(heads):
                now = jnp.where(limit <= row + i * KB, s[part(h, i)], -jnp.inf)
                scores[0, part(h, i), :] = now
                high[part(h, i), :] = jnp.maximum(now[:, :HD], now[:, HD:])

        @pl.loop(0, n)
        def _(e):
            block_copy(slot, 0, e).wait()

        @pl.loop(1, chunks)
        def _(c):
            s = score(pl.multiple_of(c * CHUNK, CHUNK))
            codes = []
            for p in range(blocks):
                e = (c - 1) * 4 + p
                codes.append(jnp.where(e < n, plan[b, e] // 256, 0))
            for i in range(blocks):
                shift = jnp.zeros((1, CHUNK), jnp.float32)
                for p in range(blocks):
                    absent = jnp.where((codes[p] >> i) & 1 != 0, jnp.float32(0), -jnp.inf)
                    shift = jnp.where(place == p, absent, shift)
                for h in range(heads):
                    now = s[part(h, i)] + shift
                    scores[c, part(h, i), :] = now
                    high[part(h, i), :] = jnp.maximum(high[part(h, i), :], jnp.maximum(now[:, :HD], now[:, HD:]))

        for h in range(heads):
            for i in range(blocks):
                top = jnp.max(high[part(h, i), :], axis=1, keepdims=True)
                high[part(h, i), :] = jnp.broadcast_to(top, (KB, HD))
        total[...] = jnp.zeros_like(total)

        @pl.loop(0, chunks)
        def _(c):
            for h in range(heads):
                for i in range(blocks):
                    top = high[part(h, i), :]
                    left = jnp.exp(scores[c, part(h, i), :HD] - top)
                    right = jnp.exp(scores[c, part(h, i), HD:] - top)
                    scores[c, part(h, i), :HD] = left
                    scores[c, part(h, i), HD:] = right
                    total[part(h, i), :] += left + right

        again = jnp.int32(0)
        for i in range(blocks):
            again += plan[MORE + b * 4 + i, REPEATS]

        def self_part(h, i):
            return jnp.where(col == row + i * KB, scores[0, part(h, i), :], 0.0)

        @pl.when(again > 0)
        def _():
            for h in range(heads):
                for i in range(blocks):
                    e = self_part(h, i)
                    times = plan[MORE + b * 4 + i, REPEATS].astype(jnp.float32)
                    total[part(h, i), :] += times * (e[:, :HD] + e[:, HD:])

        for h in range(heads):
            for i in range(blocks):
                share = 1.0 / jnp.sum(total[part(h, i), :], axis=1, keepdims=True)
                total[part(h, i), :] = jnp.broadcast_to(share, (KB, HD))
        acc[...] = jnp.zeros_like(acc)

        @pl.when(again > 0)
        def _():
            for h in range(heads):
                for i in range(blocks):
                    share = total[part(h, i), :]
                    e = self_part(h, i)
                    weight = jnp.concatenate([e[:, :HD] * share, e[:, HD:] * share], axis=1)
                    times = plan[MORE + b * 4 + i, REPEATS].astype(jnp.float32)
                    acc[part(h, i), :] = times * jnp.dot(
                        weight.astype(jnp.bfloat16), held[:SPAN, HD:], preferred_element_type=jnp.float32)

        @pl.loop(0, chunks)
        def _(c):
            share = total[...]
            weight = jnp.concatenate([scores[c, :, :HD] * share, scores[c, :, HD:] * share], axis=1)
            acc[...] += jnp.dot(weight.astype(jnp.bfloat16),
                                held[pl.ds(pl.multiple_of(c * CHUNK, CHUNK), CHUNK), HD:],
                                preferred_element_type=jnp.float32)

        pos = kv * SPAN + lax.broadcasted_iota(jnp.int32, (SPAN, HD), 0)
        for h in range(heads):
            done = jnp.where(pos < lengths[b], acc[h * SPAN:(h + 1) * SPAN, :], 0.0)
            out[slot, :, h * HD:(h + 1) * HD] = done.astype(jnp.bfloat16)

    @pl.loop(slots, SEQS)
    def _(slot):
        out[slot] = jnp.zeros((SPAN, 2 * HD), jnp.bfloat16)

    @pl.when(slots > 0)
    def _():
        fetch(jnp.int32(0))

    @pl.loop(0, slots)
    def _(slot):
        @pl.when(slot + 1 < slots)
        def _():
            fetch(slot + 1)

        compute(slot)


def attend(lengths, plan, q, cache):
    most = NZ * NX * (SPAN // KB)
    rows = 2 * SPAN
    return pl.pallas_call(
        attend_kernel,
        name="attend",
        out_shape=jax.ShapeDtypeStruct((SEQS, SPAN, 2 * HD), jnp.bfloat16),
        in_specs=[SMEM, SMEM, VMEM, ANY],
        out_specs=VMEM,
        scratch_shapes=[
            pltpu.VMEM((2, SPAN + most * KB, 2 * HD), jnp.bfloat16),
            pltpu.VMEM((1 + most // 4, rows, CHUNK), jnp.float32),
            pltpu.VMEM((rows, HD), jnp.float32),
            pltpu.VMEM((rows, HD), jnp.float32),
            pltpu.VMEM((rows, HD), jnp.float32),
            pltpu.SemaphoreType.DMA((2,)),
            pltpu.SemaphoreType.DMA((2,)),
        ],
    )(lengths, plan, q, cache)


def mix_kernel(reach, lengths, own, columns, out_w, out, groups, own_w, acc, load_sem, next_recv,
               prev_recv, core_recv, sent):
    kv, tp = lax.axis_index("kv"), lax.axis_index("tp")
    z = kv // NX
    y, core = tp // 2, tp % 2
    y_next, y_prev, y_far = (y + 1) % NY, (y + NY - 1) % NY, (y + 2) % NY
    after, before = {"tp": y_next * 2 + core}, {"tp": y_prev * 2 + core}
    partner = {"tp": y * 2 + 1 - core}
    half = SPAN // 2

    load = pltpu.make_async_copy(out_w.at[:, pl.ds(pl.multiple_of(tp * SPAN, SPAN), SPAN)], own_w, load_sem)
    load.start()
    barrier = pltpu.get_barrier_semaphore()
    for d in (after, before, partner):
        pl.semaphore_signal(barrier, inc=1, device_id=d, device_id_type=MESH)
    load.wait()
    pl.semaphore_wait(barrier, 3)

    def piece(owner_y, owner_core, slot, h):
        return groups.at[owner_y * 2 + owner_core, slot, pl.ds(h * half, half)]

    def copy(src, dst, send_sem, recv_sem, device):
        return pltpu.make_async_remote_copy(
            src_ref=src, dst_ref=dst, send_sem=send_sem, recv_sem=recv_sem,
            device_id=device, device_id_type=MESH)

    def mine(slot, h):
        return own.at[slot, pl.ds(h * half, half)]

    def to_next(slot, h):
        return copy(mine(slot, h), piece(y, core, slot, h), sent.at[slot], next_recv.at[h, slot], after)

    def to_prev(slot, h):
        return copy(mine(slot, h), piece(y, core, slot, h), sent.at[slot], prev_recv.at[h, slot], before)

    def on_next(slot):
        here = piece(y_prev, core, slot, 0)
        return copy(here, here, sent.at[slot], next_recv.at[2, slot], after)

    def on_prev(slot):
        here = piece(y_next, core, slot, 1)
        return copy(here, here, sent.at[slot], prev_recv.at[2, slot], before)

    def across(stage, owner_y, slot, h, src=None):
        here = piece(owner_y, core, slot, h)
        return copy(here if src is None else src, here, sent.at[slot], core_recv.at[stage, slot], partner)

    def crossed(stage, slot):
        both = groups.at[0, slot]
        copy(both, both, sent.at[slot], core_recv.at[stage, slot], partner).wait_recv()

    def each(body):
        for slot in range(SEQS):
            @pl.when(z <= reach[slot])
            def _(slot=slot):
                body(slot)

    def product(rows, weight):
        part = jnp.dot(rows, weight, preferred_element_type=jnp.float32)
        return part.astype(jnp.bfloat16).astype(jnp.float32)

    def add(slot, owner_y, owner_core):
        g = owner_y * 2 + owner_core
        acc[slot] += product(groups[g, slot], columns[g])

    def begin(slot):
        to_next(slot, 0).start()
        to_prev(slot, 1).start()
        to_next(slot, 1).start()
        to_prev(slot, 0).start()
        for h in range(2):
            across(0, y, slot, h, mine(slot, h)).start()

    def first(slot):
        acc[slot] = product(own[slot], own_w[...])

    def relay(slot):
        to_next(slot, 0).wait_recv()
        on_next(slot).start()
        across(1, y_prev, slot, 0).start()
        to_prev(slot, 1).wait_recv()
        on_prev(slot).start()
        across(2, y_next, slot, 1).start()
        to_next(slot, 1).wait_recv()
        across(1, y_prev, slot, 1).start()
        to_prev(slot, 0).wait_recv()
        across(2, y_next, slot, 0).start()

    def near(slot):
        crossed(0, slot)
        for owner_y, owner_core in ((y, 1 - core), (y_prev, core), (y_next, core)):
            add(slot, owner_y, owner_core)

    def far(slot):
        on_next(slot).wait_recv()
        across(3, y_far, slot, 0).start()
        on_prev(slot).wait_recv()
        across(3, y_far, slot, 1).start()
        for stage, owner_y in ((1, y_prev), (2, y_next)):
            crossed(stage, slot)
            add(slot, owner_y, 1 - core)
        add(slot, y_far, core)

    def last(slot):
        crossed(3, slot)
        add(slot, y_far, 1 - core)

    def finish(slot):
        all_sent = groups.at[pl.ds(0, 7), slot]
        copy(all_sent, all_sent, sent.at[slot], core_recv.at[0, slot], partner).wait_send()

    each(begin)
    acc[...] = jnp.zeros_like(acc)
    each(first)

    def both(slot):
        relay(slot)
        near(slot)

    each(both)
    each(far)
    each(last)
    for b in range(SEQS):
        slot = jnp.int32(0)
        for o in range(SEQS):
            if o < b:
                slot += (lengths[o] >= lengths[b]).astype(jnp.int32)
            elif o > b:
                slot += (lengths[o] > lengths[b]).astype(jnp.int32)
        out[b] = acc[slot].astype(jnp.bfloat16)
    each(finish)


def mix(reach, lengths, own, columns, out_weight):
    dma = pltpu.SemaphoreType.DMA
    return pl.pallas_call(
        lambda *refs: mix_kernel(reach, *refs),
        name="mix",
        out_shape=jax.ShapeDtypeStruct((SEQS, SPAN, SPAN), jnp.bfloat16),
        in_specs=[SMEM, VMEM, VMEM, ANY],
        out_specs=VMEM,
        scratch_shapes=[
            pltpu.VMEM((NTP, SEQS, SPAN, 2 * HD), jnp.bfloat16),
            pltpu.VMEM((SPAN, SPAN), jnp.bfloat16),
            pltpu.VMEM((SEQS, SPAN, SPAN), jnp.float32),
            dma,
            dma((3, SEQS)),
            dma((3, SEQS)),
            dma((4, SEQS)),
            dma((SEQS,)),
        ],
        compiler_params=pltpu.CompilerParams(
            collective_id=2 if reach == REACH else 3, has_side_effects=True
        ),
    )(lengths, own, columns, out_weight)


def shards(inputs, query_weight, key_weight, value_weight, out_weight, chosen, lengths):
    def rest(reach):
        cache, columns, queries, plan = spread(
            reach, lengths, chosen, inputs, query_weight, key_weight, value_weight, out_weight)
        attended = attend(lengths, plan, queries, cache)
        return mix(reach, lengths, attended, columns, out_weight)

    score = jnp.where(lengths > 3072, 6, jnp.where(lengths > 2048, 3, jnp.where(lengths > 1024, 2, 0)))
    near = jnp.sum(score) < 12
    return lax.cond(near, lambda: rest(NEAR_REACH), lambda: rest(REACH))


def solution(mesh):
    placed = (
        P(None, "kv", None),
        P(None, "tp"),
        P(None, "tp"),
        P(None, "tp"),
        P("tp", None),
        P(None, "kv", None),
        P(),
    )
    return jax.shard_map(
        shards, mesh=mesh, in_specs=placed, out_specs=P(None, "kv", "tp"), check_vma=False
    )
```

```python
import jax
import jax.numpy as jnp
from jax import lax
from jax.experimental import pallas as pl
from jax.experimental.pallas import tpu as pltpu
from jax.sharding import PartitionSpec as P

HD = 128
KB = 64
TOPK = 32
SEQS = 4
SPAN = 256
MODEL = 2048
NZ, NX, NY = 8, 4, 4
NTP = 8
REACH = (7, 5, 3, 2)
NEAR_REACH = (7, 2, 1, 0)
LANES = 128
MORE = 8
COUNT = 124
REPEATS, LOCAL, LIVE, ORDER = 0, 1, 2, 3
CHUNK = 256
MESH = pl.DeviceIdType.MESH
ANY = pl.BlockSpec(memory_space=pl.ANY)
SMEM = pl.BlockSpec(memory_space=pltpu.SMEM)
VMEM = pl.BlockSpec(memory_space=pltpu.VMEM)


def sequence_of(slot, lengths):
    size = [lengths[b] for b in range(SEQS)]
    found = jnp.int32(0)
    for b in range(SEQS):
        rank = jnp.int32(0)
        for o in range(SEQS):
            if o < b:
                rank += (size[o] >= size[b]).astype(jnp.int32)
            elif o > b:
                rank += (size[o] > size[b]).astype(jnp.int32)
        found += jnp.where(rank == slot, b, 0)
    return found


def make_plan(kv, lengths, chosen, plan, named, packed):
    named[...] = jnp.full(named.shape, -1, jnp.int32)
    for b in range(SEQS):
        named[b * 4:(b + 1) * 4, :TOPK] = chosen[b]
    block = named[...]
    lane = lax.broadcasted_iota(jnp.int32, block.shape, 1)
    row = lax.broadcasted_iota(jnp.int32, block.shape, 0)
    i = row % 4
    length = jnp.full(block.shape, lengths[0])
    for b in range(1, SEQS):
        length = jnp.where(row // 4 == b, lengths[b], length)
    member = jnp.zeros(block.shape, jnp.int32)
    for e in range(TOPK):
        member |= (block[:, e:e + 1] == lane).astype(jnp.int32)
    member = jnp.where((kv * 4 + i) * KB < length, member, 0)
    repeats = jnp.sum((block == kv * 4 + i).astype(jnp.int32), axis=1, keepdims=True) - 1
    here = lane - kv * 4
    inside = (here >= 0) & (here < 4)
    local = jnp.sum(jnp.where(inside, member << jnp.where(inside, here, 0), 0), axis=1, keepdims=True)
    named[...] = jnp.where(here < 0, member << i, 0)
    live = jnp.int32(0)
    for b in range(SEQS):
        live += (lengths[b] > kv * SPAN).astype(jnp.int32)
    more = jnp.where(lane == REPEATS, repeats, jnp.where(lane == LOCAL, local, live))
    for j in range(SEQS):
        more = jnp.where(lane == ORDER + j, sequence_of(j, lengths), more)
    plan[MORE:, :] = more

    packed[...] = jnp.zeros(packed.shape, jnp.int32)
    for b in range(SEQS):
        packed[b:b + 1, :] = jnp.sum(named[b * 4:(b + 1) * 4, :], axis=0, keepdims=True)
    code = packed[...]
    lane = lax.broadcasted_iota(jnp.int32, code.shape, 1)
    held = (code != 0).astype(jnp.int32)
    code = lane + 256 * code
    steps = (1, 2, 4, 8, 16, 32, 64)
    upto = held
    for s in steps:
        upto += jnp.where(lane >= s, pltpu.roll(upto, s, 1), 0)
    count = jnp.sum(held, axis=1, keepdims=True)
    gap = lane - (upto - 1)
    for s in steps:
        there = pltpu.roll(code, LANES - s, 1)
        there_gap = pltpu.roll(gap, LANES - s, 1)
        take = (pltpu.roll(held, LANES - s, 1) != 0) & ((there_gap & s) != 0)
        stay = (held != 0) & ((gap & s) == 0)
        code = jnp.where(take, there, code)
        gap = jnp.where(take, there_gap, gap)
        held = (take | stay).astype(jnp.int32)
    plan[:MORE, :] = jnp.where(lane == COUNT, count, code)


def spread_kernel(reach, lengths, chosen, inputs, query_w, key_w, value_w, out_w,
                  cache, columns, q_out, plan, held, rows_in, q_weights, kv_weights, projected,
                  named, packed, load_sem, store_sem, recv, up_sem, beside_sem, once_sem):
    kv, tp = lax.axis_index("kv"), lax.axis_index("tp")
    z, x = kv // NX, kv % NX
    right = {"kv": z * NX + (x + 1) % NX}
    left = {"kv": z * NX + (x + NX - 1) % NX}
    x_right, x_left, x_far = (x + 1) % NX, (x + NX - 1) % NX, (x + 2) % NX
    half = SPAN // 2
    TO_TOP, RELAY_UP, RELAY_DOWN, W_SEND, W_RECV = range(5)
    COLUMN, LEFT, RIGHT, LATE = 0, 2, 3, 4

    loads = [
        pltpu.make_async_copy(key_w, kv_weights.at[:, pl.ds(0, HD)], load_sem.at[0]),
        pltpu.make_async_copy(value_w, kv_weights.at[:, pl.ds(HD, HD)], load_sem.at[1]),
    ]
    loads += [pltpu.make_async_copy(inputs.at[b], rows_in.at[b], load_sem.at[2 + b]) for b in range(SEQS)]
    load_q = pltpu.make_async_copy(query_w, q_weights, load_sem.at[2 + SEQS])
    for load in loads:
        load.start()
    load_q.start()

    above = {"kv": (z + 1) % NZ * NX + x}
    below = {"kv": (z + NZ - 1) % NZ * NX + x}
    top = {"kv": (NZ - 1) * NX + x}

    barrier = pltpu.get_barrier_semaphore()

    def greet(device):
        pl.semaphore_signal(barrier, inc=1, device_id=device, device_id_type=MESH)

    for d in (above, below, right, left):
        greet(d)
    for d in range(1, NTP):
        greet({"tp": (tp + d) % NTP})
    low = (z >= 1) & (z <= 2)

    @pl.when(low)
    def _():
        greet(top)

    @pl.when(z == NZ - 1)
    def _():
        for w in (1, 2):
            greet({"kv": w * NX + x})

    loads[0].wait()
    loads[1].wait()
    for b in range(SEQS):
        loads[2 + b].wait()
        projected[b] = jnp.dot(rows_in[b], kv_weights[...], preferred_element_type=jnp.float32).astype(jnp.bfloat16)
    for slot in range(SEQS):
        held[slot, pl.ds(pl.multiple_of(kv * SPAN, SPAN), SPAN), :] = projected[sequence_of(slot, lengths)]

    pl.semaphore_wait(barrier, 4 + NTP - 1 + low.astype(jnp.int32) + z // (NZ - 1) * 2)

    def piece(slot, owner_z, owner_x, h):
        first = pl.multiple_of((owner_z * NX + owner_x) * SPAN + h * half, half)
        return held.at[slot, pl.ds(first, half)]

    def mine(slot, h):
        return piece(slot, z, x, h)

    def store(slot, w):
        span = pl.ds(pl.multiple_of(w * NX * SPAN, NX * SPAN), NX * SPAN)
        return pltpu.make_async_copy(held.at[slot, span], cache.at[slot, span], store_sem.at[row(slot, w)])

    def row(slot, w):
        return sum(reach[o] + 1 for o in range(slot)) + w

    def send(src, sem, slot, owner_z, owner_x, h, kind, device):
        return pltpu.make_async_remote_copy(
            src_ref=src, dst_ref=piece(slot, owner_z, owner_x, h), send_sem=sem,
            recv_sem=recv.at[row(slot, owner_z), kind],
            device_id=device, device_id_type=MESH)

    def arrived(slot, w, kind):
        size = SPAN * 2 if kind == LATE else half
        there = held.at[slot, pl.ds(0, size)]
        pltpu.make_async_remote_copy(
            src_ref=there, dst_ref=there, send_sem=up_sem.at[row(slot, w)],
            recv_sem=recv.at[row(slot, w), kind], device_id=right, device_id_type=MESH).wait_recv()

    def sent(slot, sem, pieces):
        there = held.at[slot, pl.ds(0, pieces * half)]
        pltpu.make_async_remote_copy(
            src_ref=there, dst_ref=there, send_sem=sem, recv_sem=recv.at[0, 0],
            device_id=right, device_id_type=MESH).wait_send()

    def goes_up(slot, d):
        climb = 3 if slot == 0 else NZ
        return (z + 1 <= reach[slot]) & (d <= climb)

    columns_of = (x, x_left, x_far, x_right)

    def whole(d):
        return (d == z) & ((z <= 2) | (z >= 6))

    def relay(c, h, kind):
        src = piece(0, 0, columns_of[c], h)

        @pl.when(z < (3 if c == 0 else 2))
        def _():
            send(src, once_sem.at[RELAY_UP], 0, 0, columns_of[c], h, kind, above).start()

        @pl.when((z == 0) | (z >= (6 if c == 0 else 7)))
        def _():
            send(src, once_sem.at[RELAY_DOWN], 0, 0, columns_of[c], h, kind, below).start()

    def plain(slot, d):
        return jnp.logical_not(whole(d)) if slot == 0 else z >= 0

    def onward(slot, d):
        if slot > 0:
            return goes_up(slot, d), z < 0
        chained = jnp.logical_not(whole(d))
        return chained & goes_up(slot, d), chained & (d >= 6)

    def along(slot, d, h):
        w = z - d
        src = piece(slot, w, x, h)
        up, down = onward(slot, d)

        @pl.when(up)
        def _():
            send(src, up_sem.at[row(slot, w)], slot, w, x, h, COLUMN + h, above).start()

        if slot == 0:
            @pl.when(down)
            def _():
                send(src, up_sem.at[row(slot, w)], slot, w, x, h, COLUMN + h, below).start()

            @pl.when(whole(d))
            def _():
                relay(0, h, COLUMN + h)

        @pl.when(plain(slot, d) | (z == 0))
        def _():
            sem = beside_sem.at[row(slot, w)]
            send(src, sem, slot, w, x, h, LEFT if h == 0 else LATE, right).start()
            send(src, sem, slot, w, x, h, LATE if h == 0 else RIGHT, left).start()

    def to_top(h):
        return send(mine(0, h), once_sem.at[TO_TOP], 0, z, x, h, COLUMN + h, top)

    def each(body, slots=range(SEQS)):
        for slot in slots:
            @pl.when(z <= reach[slot])
            def _(slot=slot):
                body(slot)

    def distance(t):
        return t % 2 * ((t + 1) // 2) + (1 - t % 2) * ((NZ - t // 2) % NZ)

    def around(t, slots=range(SEQS)):
        d = distance(t)
        w = z - d

        def passing(slot):
            sem = beside_sem.at[row(slot, w)]
            send(piece(slot, w, x_left, 0), sem, slot, w, x_left, 0, LATE, right).start()
            send(piece(slot, w, x_right, 1), sem, slot, w, x_right, 1, LATE, left).start()

        def body(slot):
            arrived(slot, w, LEFT)
            arrived(slot, w, RIGHT)
            if slot == 0:
                @pl.when(plain(slot, d) | (z == 0))
                def _():
                    passing(slot)

                @pl.when(whole(d))
                def _():
                    relay(1, 0, LEFT)
                    relay(3, 1, RIGHT)
            else:
                passing(slot)

        each(body, slots)

    def tail(t):
        d = distance(t)
        late = ((1, 1), (3, 0), (2, 0), (2, 1))

        @pl.when(whole(d) & (z <= reach[0]))
        def _():
            arrived(0, 0, LATE)
            for c, h in late:
                relay(c, h, LATE)

    def column(t):
        d = distance(t)

        def body(slot):
            for h in range(2):
                arrived(slot, z - d, COLUMN + h)
                along(slot, d, h)

        each(body)

    def settle(t):
        d = distance(t)
        w = z - d

        def body(slot):
            if slot == 0:
                @pl.when(plain(slot, d))
                def _():
                    arrived(slot, w, LATE)
            else:
                arrived(slot, w, LATE)
            store(slot, w).start()

        each(body)

    def finish(t):
        d = distance(t)
        w = z - d

        def body(slot):
            up, down = onward(slot, d)

            @pl.when(up | down)
            def _():
                sent(slot, up_sem.at[row(slot, w)], 2)

            @pl.when(plain(slot, d) | (z == 0))
            def _():
                sent(slot, beside_sem.at[row(slot, w)], 6)

            store(slot, w).wait()

        each(body)

    def column_copy(d):
        peer = (tp + d) % NTP
        first = pl.multiple_of(peer * SPAN, SPAN)
        return pltpu.make_async_remote_copy(
            src_ref=out_w.at[:, pl.ds(first, SPAN)], dst_ref=columns.at[tp],
            send_sem=once_sem.at[W_SEND], recv_sem=once_sem.at[W_RECV],
            device_id={"tp": peer}, device_id_type=MESH)

    def begin(slot):
        for h in range(2):
            along(slot, 0, h)

    @pl.when(low)
    def _():
        for h in range(2):
            to_top(h).start()

    each(begin, (0, 1))

    around(0, (0,))
    each(begin, (2, 3))
    for d in range(1, NTP):
        column_copy(d).start()

    load_q.wait()

    @pl.loop(1, NZ)
    def _(t):
        @pl.when(distance(t) <= z)
        def _():
            column(t)

        @pl.when(t <= SEQS)
        def _():
            q_out[t - 1] = jnp.dot(
                rows_in[t - 1], q_weights[...], preferred_element_type=jnp.float32).astype(jnp.bfloat16)

        @pl.when(t == SEQS + 1)
        def _():
            make_plan(kv, lengths, chosen, plan, named, packed)

    tail(0)
    around(0, (1, 2, 3))

    @pl.loop(1, NZ)
    def _(t):
        @pl.when(distance(t) <= z)
        def _():
            around(t)
            tail(t)

    @pl.loop(0, NZ)
    def _(t):
        @pl.when(distance(t) <= z)
        def _():
            settle(t)

    @pl.loop(0, NZ)
    def _(t):
        @pl.when(distance(t) <= z)
        def _():
            finish(t)

    @pl.when(low)
    def _():
        sent(0, once_sem.at[TO_TOP], 2)

    climbs = z <= reach[0]

    @pl.when(climbs & (z < 2))
    def _():
        sent(0, once_sem.at[RELAY_UP], 8)

    @pl.when(climbs & (z == 2))
    def _():
        sent(0, once_sem.at[RELAY_UP], 2)

    @pl.when(climbs & ((z == 0) | (z == 7)))
    def _():
        sent(0, once_sem.at[RELAY_DOWN], 8)

    @pl.when(climbs & (z == 6))
    def _():
        sent(0, once_sem.at[RELAY_DOWN], 2)

    others = columns.at[pl.ds(0, NTP - 1)]
    pltpu.make_async_remote_copy(
        src_ref=others, dst_ref=others, send_sem=once_sem.at[W_SEND], recv_sem=once_sem.at[W_RECV],
        device_id=right, device_id_type=MESH).wait()


def spread(reach, lengths, chosen, inputs, query_weight, key_weight, value_weight, out_weight):
    dma = pltpu.SemaphoreType.DMA
    named = SEQS * (SPAN // KB)
    rows = sum(r + 1 for r in reach)
    return pl.pallas_call(
        lambda *refs: spread_kernel(reach, *refs),
        name="spread",
        out_shape=(
            jax.ShapeDtypeStruct((SEQS, NZ * NX * SPAN, 2 * HD), jnp.bfloat16),
            jax.ShapeDtypeStruct((NTP, SPAN, SPAN), jnp.bfloat16),
            jax.ShapeDtypeStruct((SEQS, SPAN, 2 * HD), jnp.bfloat16),
            jax.ShapeDtypeStruct((MORE + named, LANES), jnp.int32),
        ),
        in_specs=[SMEM, VMEM] + [ANY] * 5,
        out_specs=(ANY, ANY, VMEM, VMEM),
        scratch_shapes=[
            pltpu.VMEM((SEQS, NZ * NX * SPAN, 2 * HD), jnp.bfloat16),
            pltpu.VMEM((SEQS, SPAN, MODEL), jnp.bfloat16),
            pltpu.VMEM((MODEL, 2 * HD), jnp.bfloat16),
            pltpu.VMEM((MODEL, 2 * HD), jnp.bfloat16),
            pltpu.VMEM((SEQS, SPAN, 2 * HD), jnp.bfloat16),
            pltpu.VMEM((named, LANES), jnp.int32),
            pltpu.VMEM((MORE, LANES), jnp.int32),
            dma((SEQS + 3,)),
            dma((rows,)),
            dma((rows, 5)),
            dma((rows,)),
            dma((rows,)),
            dma((5,)),
        ],
        compiler_params=pltpu.CompilerParams(
            collective_id=0 if reach == REACH else 1, has_side_effects=True
        ),
    )(lengths, chosen, inputs, query_weight, key_weight, value_weight, out_weight)


def attend_kernel(lengths, plan, q, cache, out, keys, scores, high, total, acc, own_sems, sems):
    kv = lax.axis_index("kv")
    slots = plan[MORE, LIVE]
    blocks = SPAN // KB
    heads = 2

    def sequence(slot):
        b = plan[MORE, ORDER + slot]
        return b, plan[b, COUNT]

    def own_copy(slot):
        span = pl.ds(pl.multiple_of(kv * SPAN, SPAN), SPAN)
        return pltpu.make_async_copy(
            cache.at[slot, span], keys.at[slot % 2, pl.ds(0, SPAN)], own_sems.at[slot % 2])

    def block_copy(slot, block, e):
        row = pl.multiple_of(block * KB, KB)
        to = pl.multiple_of(SPAN + e * KB, KB)
        return pltpu.make_async_copy(
            cache.at[slot, pl.ds(row, KB)], keys.at[slot % 2, pl.ds(to, KB)], sems.at[slot % 2])

    def fetch(slot):
        b, n = sequence(slot)
        own_copy(slot).start()

        @pl.loop(0, n)
        def _(e):
            block_copy(slot, plan[b, e] % 256, e).start()

        past = pl.ds(pl.multiple_of(SPAN + n * KB, KB), 3 * KB)
        keys[slot % 2, past, :] = jnp.zeros((3 * KB, 2 * HD), jnp.bfloat16)

    def part(h, i):
        return slice(h * SPAN + i * KB, h * SPAN + (i + 1) * KB)

    def compute(slot):
        b, n = sequence(slot)
        held = keys.at[slot % 2]
        chunks = 1 + (n + 3) // 4
        own_copy(slot).wait()
        both = q[b]
        stacked = jnp.concatenate([both[:, :HD], both[:, HD:]], axis=0)
        lane = lax.broadcasted_iota(jnp.int32, (1, CHUNK), 1)
        place = lane // KB

        def score(first):
            return lax.dot_general(stacked, held[pl.ds(first, CHUNK), :HD], (((1,), (1,)), ((), ())),
                                   preferred_element_type=jnp.float32) * (HD ** -0.5)

        s = score(0)
        col = lax.broadcasted_iota(jnp.int32, (KB, CHUNK), 1)
        row = lax.broadcasted_iota(jnp.int32, (KB, CHUNK), 0)
        for i in range(blocks):
            bits = plan[MORE + b * 4 + i, LOCAL] | (1 << i)
            named = jnp.zeros((1, CHUNK), jnp.int32)
            for p in range(blocks):
                named = jnp.where(place == p, (bits >> p) & 1, named)
            limit = jnp.where(named != 0, lane, SPAN)
            for h in range(heads):
                now = jnp.where(limit <= row + i * KB, s[part(h, i)], -jnp.inf)
                scores[0, part(h, i), :] = now
                high[part(h, i), :] = jnp.maximum(now[:, :HD], now[:, HD:])

        @pl.loop(0, n)
        def _(e):
            block_copy(slot, 0, e).wait()

        @pl.loop(1, chunks)
        def _(c):
            s = score(pl.multiple_of(c * CHUNK, CHUNK))
            codes = []
            for p in range(blocks):
                e = (c - 1) * 4 + p
                codes.append(jnp.where(e < n, plan[b, e] // 256, 0))
            for i in range(blocks):
                shift = jnp.zeros((1, CHUNK), jnp.float32)
                for p in range(blocks):
                    absent = jnp.where((codes[p] >> i) & 1 != 0, jnp.float32(0), -jnp.inf)
                    shift = jnp.where(place == p, absent, shift)
                for h in range(heads):
                    now = s[part(h, i)] + shift
                    scores[c, part(h, i), :] = now
                    high[part(h, i), :] = jnp.maximum(high[part(h, i), :], jnp.maximum(now[:, :HD], now[:, HD:]))

        for h in range(heads):
            for i in range(blocks):
                top = jnp.max(high[part(h, i), :], axis=1, keepdims=True)
                high[part(h, i), :] = jnp.broadcast_to(top, (KB, HD))
        total[...] = jnp.zeros_like(total)

        @pl.loop(0, chunks)
        def _(c):
            for h in range(heads):
                for i in range(blocks):
                    top = high[part(h, i), :]
                    left = jnp.exp(scores[c, part(h, i), :HD] - top)
                    right = jnp.exp(scores[c, part(h, i), HD:] - top)
                    scores[c, part(h, i), :HD] = left
                    scores[c, part(h, i), HD:] = right
                    total[part(h, i), :] += left + right

        again = jnp.int32(0)
        for i in range(blocks):
            again += plan[MORE + b * 4 + i, REPEATS]

        def self_part(h, i):
            return jnp.where(col == row + i * KB, scores[0, part(h, i), :], 0.0)

        @pl.when(again > 0)
        def _():
            for h in range(heads):
                for i in range(blocks):
                    e = self_part(h, i)
                    times = plan[MORE + b * 4 + i, REPEATS].astype(jnp.float32)
                    total[part(h, i), :] += times * (e[:, :HD] + e[:, HD:])

        for h in range(heads):
            for i in range(blocks):
                share = 1.0 / jnp.sum(total[part(h, i), :], axis=1, keepdims=True)
                total[part(h, i), :] = jnp.broadcast_to(share, (KB, HD))
        acc[...] = jnp.zeros_like(acc)

        @pl.when(again > 0)
        def _():
            for h in range(heads):
                for i in range(blocks):
                    share = total[part(h, i), :]
                    e = self_part(h, i)
                    weight = jnp.concatenate([e[:, :HD] * share, e[:, HD:] * share], axis=1)
                    times = plan[MORE + b * 4 + i, REPEATS].astype(jnp.float32)
                    acc[part(h, i), :] = times * jnp.dot(
                        weight.astype(jnp.bfloat16), held[:SPAN, HD:], preferred_element_type=jnp.float32)

        @pl.loop(0, chunks)
        def _(c):
            share = total[...]
            weight = jnp.concatenate([scores[c, :, :HD] * share, scores[c, :, HD:] * share], axis=1)
            acc[...] += jnp.dot(weight.astype(jnp.bfloat16),
                                held[pl.ds(pl.multiple_of(c * CHUNK, CHUNK), CHUNK), HD:],
                                preferred_element_type=jnp.float32)

        pos = kv * SPAN + lax.broadcasted_iota(jnp.int32, (SPAN, HD), 0)
        for h in range(heads):
            done = jnp.where(pos < lengths[b], acc[h * SPAN:(h + 1) * SPAN, :], 0.0)
            out[slot, :, h * HD:(h + 1) * HD] = done.astype(jnp.bfloat16)

    @pl.loop(slots, SEQS)
    def _(slot):
        out[slot] = jnp.zeros((SPAN, 2 * HD), jnp.bfloat16)

    @pl.when(slots > 0)
    def _():
        fetch(jnp.int32(0))

    @pl.loop(0, slots)
    def _(slot):
        @pl.when(slot + 1 < slots)
        def _():
            fetch(slot + 1)

        compute(slot)


def attend(lengths, plan, q, cache):
    most = NZ * NX * (SPAN // KB)
    rows = 2 * SPAN
    return pl.pallas_call(
        attend_kernel,
        name="attend",
        out_shape=jax.ShapeDtypeStruct((SEQS, SPAN, 2 * HD), jnp.bfloat16),
        in_specs=[SMEM, SMEM, VMEM, ANY],
        out_specs=VMEM,
        scratch_shapes=[
            pltpu.VMEM((2, SPAN + most * KB, 2 * HD), jnp.bfloat16),
            pltpu.VMEM((1 + most // 4, rows, CHUNK), jnp.float32),
            pltpu.VMEM((rows, HD), jnp.float32),
            pltpu.VMEM((rows, HD), jnp.float32),
            pltpu.VMEM((rows, HD), jnp.float32),
            pltpu.SemaphoreType.DMA((2,)),
            pltpu.SemaphoreType.DMA((2,)),
        ],
    )(lengths, plan, q, cache)


def mix_kernel(reach, lengths, attended, columns_in, out_w, out, groups, own, columns, own_w, acc,
               load_sem, next_recv, prev_recv, core_recv, sent):
    kv, tp = lax.axis_index("kv"), lax.axis_index("tp")
    z = kv // NX
    y, core = tp // 2, tp % 2
    y_next, y_prev, y_far = (y + 1) % NY, (y + NY - 1) % NY, (y + 2) % NY
    after, before = {"tp": y_next * 2 + core}, {"tp": y_prev * 2 + core}
    partner = {"tp": y * 2 + 1 - core}
    half = SPAN // 2

    barrier = pltpu.get_barrier_semaphore()
    for d in (after, before, partner):
        pl.semaphore_signal(barrier, inc=1, device_id=d, device_id_type=MESH)
    my_columns = out_w.at[:, pl.ds(pl.multiple_of(tp * SPAN, SPAN), SPAN)]
    loads = (
        pltpu.make_async_copy(attended, own, load_sem.at[0]),
        pltpu.make_async_copy(my_columns, own_w, load_sem.at[1]),
        pltpu.make_async_copy(columns_in, columns, load_sem.at[2]),
    )
    for load in loads:
        load.start()
    loads[0].wait()
    pl.semaphore_wait(barrier, 3)

    def piece(owner_y, owner_core, slot, h):
        return groups.at[owner_y * 2 + owner_core, slot, pl.ds(h * half, half)]

    def copy(src, dst, send_sem, recv_sem, device):
        return pltpu.make_async_remote_copy(
            src_ref=src, dst_ref=dst, send_sem=send_sem, recv_sem=recv_sem,
            device_id=device, device_id_type=MESH)

    def mine(slot, h):
        return own.at[slot, pl.ds(h * half, half)]

    def to_next(slot, h):
        return copy(mine(slot, h), piece(y, core, slot, h), sent.at[slot], next_recv.at[h, slot], after)

    def to_prev(slot, h):
        return copy(mine(slot, h), piece(y, core, slot, h), sent.at[slot], prev_recv.at[h, slot], before)

    def on_next(slot):
        here = piece(y_prev, core, slot, 0)
        return copy(here, here, sent.at[slot], next_recv.at[2, slot], after)

    def on_prev(slot):
        here = piece(y_next, core, slot, 1)
        return copy(here, here, sent.at[slot], prev_recv.at[2, slot], before)

    def across(stage, owner_y, slot, h, src=None):
        here = piece(owner_y, core, slot, h)
        return copy(here if src is None else src, here, sent.at[slot], core_recv.at[stage, slot], partner)

    def crossed(stage, slot):
        both = groups.at[0, slot]
        copy(both, both, sent.at[slot], core_recv.at[stage, slot], partner).wait_recv()

    def each(body):
        for slot in range(SEQS):
            @pl.when(z <= reach[slot])
            def _(slot=slot):
                body(slot)

    def product(rows, weight):
        part = jnp.dot(rows, weight, preferred_element_type=jnp.float32)
        return part.astype(jnp.bfloat16).astype(jnp.float32)

    def add(slot, owner_y, owner_core):
        g = owner_y * 2 + owner_core
        acc[slot] += product(groups[g, slot], columns[g])

    def begin(slot):
        to_next(slot, 0).start()
        to_prev(slot, 1).start()
        to_next(slot, 1).start()
        to_prev(slot, 0).start()
        for h in range(2):
            across(0, y, slot, h, mine(slot, h)).start()

    def first(slot):
        acc[slot] = product(own[slot], own_w[...])

    def relay(slot):
        to_next(slot, 0).wait_recv()
        on_next(slot).start()
        across(1, y_prev, slot, 0).start()
        to_prev(slot, 1).wait_recv()
        on_prev(slot).start()
        across(2, y_next, slot, 1).start()
        to_next(slot, 1).wait_recv()
        across(1, y_prev, slot, 1).start()
        to_prev(slot, 0).wait_recv()
        across(2, y_next, slot, 0).start()

    def near(slot):
        crossed(0, slot)
        for owner_y, owner_core in ((y, 1 - core), (y_prev, core), (y_next, core)):
            add(slot, owner_y, owner_core)

    def middle(slot):
        for stage, owner_y in ((1, y_prev), (2, y_next)):
            crossed(stage, slot)
            add(slot, owner_y, 1 - core)

    def far(slot):
        on_next(slot).wait_recv()
        across(3, y_far, slot, 0).start()
        on_prev(slot).wait_recv()
        across(3, y_far, slot, 1).start()
        if slot > 0:
            last(slot - 1)
        add(slot, y_far, core)

    def last(slot):
        crossed(3, slot)
        add(slot, y_far, 1 - core)

    def finish(slot):
        all_sent = groups.at[pl.ds(0, 7), slot]
        copy(all_sent, all_sent, sent.at[slot], core_recv.at[0, slot], partner).wait_send()

    each(begin)
    acc[...] = jnp.zeros_like(acc)
    loads[1].wait()
    each(first)
    loads[2].wait()

    def both(slot):
        relay(slot)
        near(slot)

    each(both)
    each(middle)
    each(far)
    for slot in range(SEQS):
        beyond = z <= reach[slot + 1] if slot + 1 < SEQS else z < 0

        @pl.when((z <= reach[slot]) & jnp.logical_not(beyond))
        def _(slot=slot):
            last(slot)

    for b in range(SEQS):
        slot = jnp.int32(0)
        for o in range(SEQS):
            if o < b:
                slot += (lengths[o] >= lengths[b]).astype(jnp.int32)
            elif o > b:
                slot += (lengths[o] > lengths[b]).astype(jnp.int32)
        out[b] = acc[slot].astype(jnp.bfloat16)
    each(finish)


def mix(reach, lengths, own, columns, out_weight):
    dma = pltpu.SemaphoreType.DMA
    return pl.pallas_call(
        lambda *refs: mix_kernel(reach, *refs),
        name="mix",
        out_shape=jax.ShapeDtypeStruct((SEQS, SPAN, SPAN), jnp.bfloat16),
        in_specs=[SMEM, ANY, ANY, ANY],
        out_specs=VMEM,
        scratch_shapes=[
            pltpu.VMEM((NTP, SEQS, SPAN, 2 * HD), jnp.bfloat16),
            pltpu.VMEM((SEQS, SPAN, 2 * HD), jnp.bfloat16),
            pltpu.VMEM((NTP, SPAN, SPAN), jnp.bfloat16),
            pltpu.VMEM((SPAN, SPAN), jnp.bfloat16),
            pltpu.VMEM((SEQS, SPAN, SPAN), jnp.float32),
            dma((3,)),
            dma((3, SEQS)),
            dma((3, SEQS)),
            dma((4, SEQS)),
            dma((SEQS,)),
        ],
        compiler_params=pltpu.CompilerParams(
            collective_id=2 if reach == REACH else 3, has_side_effects=True
        ),
    )(lengths, own, columns, out_weight)


def shards(inputs, query_weight, key_weight, value_weight, out_weight, chosen, lengths):
    def rest(reach):
        cache, columns, queries, plan = spread(
            reach, lengths, chosen, inputs, query_weight, key_weight, value_weight, out_weight)
        attended = attend(lengths, plan, queries, cache)
        return mix(reach, lengths, attended, columns, out_weight)

    score = jnp.where(lengths > 3072, 6, jnp.where(lengths > 2048, 3, jnp.where(lengths > 1024, 2, 0)))
    near = jnp.sum(score) < 12
    return lax.cond(near, lambda: rest(NEAR_REACH), lambda: rest(REACH))


def solution(mesh):
    placed = (
        P(None, "kv", None),
        P(None, "tp"),
        P(None, "tp"),
        P(None, "tp"),
        P("tp", None),
        P(None, "kv", None),
        P(),
    )
    return jax.shard_map(
        shards, mesh=mesh, in_specs=placed, out_specs=P(None, "kv", "tp"), check_vma=False
    )
```

```python
import jax
import jax.numpy as jnp
from jax import lax
from jax.experimental import pallas as pl
from jax.experimental.pallas import tpu as pltpu
from jax.sharding import PartitionSpec as P

HD = 128
KB = 64
TOPK = 32
SEQS = 4
SPAN = 256
MODEL = 2048
NZ, NX, NY = 8, 4, 4
NTP = 8
REACH = (7, 5, 3, 2)
NEAR_REACH = (7, 2, 1, 0)
LANES = 128
MORE = 8
COUNT = 124
REPEATS, LOCAL, LIVE, ORDER = 0, 1, 2, 3
CHUNK = 256
MESH = pl.DeviceIdType.MESH
ANY = pl.BlockSpec(memory_space=pl.ANY)
SMEM = pl.BlockSpec(memory_space=pltpu.SMEM)
VMEM = pl.BlockSpec(memory_space=pltpu.VMEM)


def sequence_of(slot, lengths):
    size = [lengths[b] for b in range(SEQS)]
    found = jnp.int32(0)
    for b in range(SEQS):
        rank = jnp.int32(0)
        for o in range(SEQS):
            if o < b:
                rank += (size[o] >= size[b]).astype(jnp.int32)
            elif o > b:
                rank += (size[o] > size[b]).astype(jnp.int32)
        found += jnp.where(rank == slot, b, 0)
    return found


def make_plan(kv, lengths, chosen, plan, named, packed):
    named[...] = jnp.full(named.shape, -1, jnp.int32)
    for b in range(SEQS):
        named[b * 4:(b + 1) * 4, :TOPK] = chosen[b]
    block = named[...]
    lane = lax.broadcasted_iota(jnp.int32, block.shape, 1)
    row = lax.broadcasted_iota(jnp.int32, block.shape, 0)
    i = row % 4
    length = jnp.full(block.shape, lengths[0])
    for b in range(1, SEQS):
        length = jnp.where(row // 4 == b, lengths[b], length)
    member = jnp.zeros(block.shape, jnp.int32)
    for e in range(TOPK):
        member |= (block[:, e:e + 1] == lane).astype(jnp.int32)
    member = jnp.where((kv * 4 + i) * KB < length, member, 0)
    repeats = jnp.sum((block == kv * 4 + i).astype(jnp.int32), axis=1, keepdims=True) - 1
    here = lane - kv * 4
    inside = (here >= 0) & (here < 4)
    local = jnp.sum(jnp.where(inside, member << jnp.where(inside, here, 0), 0), axis=1, keepdims=True)
    named[...] = jnp.where(here < 0, member << i, 0)
    live = jnp.int32(0)
    for b in range(SEQS):
        live += (lengths[b] > kv * SPAN).astype(jnp.int32)
    more = jnp.where(lane == REPEATS, repeats, jnp.where(lane == LOCAL, local, live))
    for j in range(SEQS):
        more = jnp.where(lane == ORDER + j, sequence_of(j, lengths), more)
    plan[MORE:, :] = more

    packed[...] = jnp.zeros(packed.shape, jnp.int32)
    for b in range(SEQS):
        packed[b:b + 1, :] = jnp.sum(named[b * 4:(b + 1) * 4, :], axis=0, keepdims=True)
    code = packed[...]
    lane = lax.broadcasted_iota(jnp.int32, code.shape, 1)
    held = (code != 0).astype(jnp.int32)
    code = lane + 256 * code
    steps = (1, 2, 4, 8, 16, 32, 64)
    upto = held
    for s in steps:
        upto += jnp.where(lane >= s, pltpu.roll(upto, s, 1), 0)
    count = jnp.sum(held, axis=1, keepdims=True)
    gap = lane - (upto - 1)
    for s in steps:
        there = pltpu.roll(code, LANES - s, 1)
        there_gap = pltpu.roll(gap, LANES - s, 1)
        take = (pltpu.roll(held, LANES - s, 1) != 0) & ((there_gap & s) != 0)
        stay = (held != 0) & ((gap & s) == 0)
        code = jnp.where(take, there, code)
        gap = jnp.where(take, there_gap, gap)
        held = (take | stay).astype(jnp.int32)
    plan[:MORE, :] = jnp.where(lane == COUNT, count, code)


def spread_kernel(reach, lengths, chosen, inputs, query_w, key_w, value_w, out_w,
                  cache, columns, q_out, plan, held, rows_in, q_weights, kv_weights, projected,
                  named, packed, load_sem, store_sem, recv, up_sem, beside_sem, once_sem):
    kv, tp = lax.axis_index("kv"), lax.axis_index("tp")
    z, x = kv // NX, kv % NX
    right = {"kv": z * NX + (x + 1) % NX}
    left = {"kv": z * NX + (x + NX - 1) % NX}
    x_right, x_left, x_far = (x + 1) % NX, (x + NX - 1) % NX, (x + 2) % NX
    half = SPAN // 2
    TO_TOP, RELAY_UP, RELAY_DOWN, W_SEND, W_RECV = range(5)
    COLUMN, LEFT, RIGHT, LATE = 0, 2, 3, 4

    loads = [
        pltpu.make_async_copy(key_w, kv_weights.at[:, pl.ds(0, HD)], load_sem.at[0]),
        pltpu.make_async_copy(value_w, kv_weights.at[:, pl.ds(HD, HD)], load_sem.at[1]),
    ]
    loads += [pltpu.make_async_copy(inputs.at[b], rows_in.at[b], load_sem.at[2 + b]) for b in range(SEQS)]
    load_q = pltpu.make_async_copy(query_w, q_weights, load_sem.at[2 + SEQS])
    for load in loads:
        load.start()
    load_q.start()

    above = {"kv": (z + 1) % NZ * NX + x}
    below = {"kv": (z + NZ - 1) % NZ * NX + x}
    top = {"kv": (NZ - 1) * NX + x}

    barrier = pltpu.get_barrier_semaphore()

    def greet(device):
        pl.semaphore_signal(barrier, inc=1, device_id=device, device_id_type=MESH)

    for d in (above, below, right, left):
        greet(d)
    for d in range(1, NTP):
        greet({"tp": (tp + d) % NTP})
    low = (z >= 1) & (z <= 2)

    @pl.when(low)
    def _():
        greet(top)

    @pl.when(z == NZ - 1)
    def _():
        for w in (1, 2):
            greet({"kv": w * NX + x})

    loads[0].wait()
    loads[1].wait()
    for b in range(SEQS):
        loads[2 + b].wait()
        projected[b] = jnp.dot(rows_in[b], kv_weights[...], preferred_element_type=jnp.float32).astype(jnp.bfloat16)
    for slot in range(SEQS):
        held[slot, pl.ds(pl.multiple_of(kv * SPAN, SPAN), SPAN), :] = projected[sequence_of(slot, lengths)]

    pl.semaphore_wait(barrier, 4 + NTP - 1 + low.astype(jnp.int32) + z // (NZ - 1) * 2)

    def piece(slot, owner_z, owner_x, h):
        first = pl.multiple_of((owner_z * NX + owner_x) * SPAN + h * half, half)
        return held.at[slot, pl.ds(first, half)]

    def mine(slot, h):
        return piece(slot, z, x, h)

    def store(slot, w):
        span = pl.ds(pl.multiple_of(w * NX * SPAN, NX * SPAN), NX * SPAN)
        return pltpu.make_async_copy(held.at[slot, span], cache.at[slot, span], store_sem.at[row(slot, w)])

    def row(slot, w):
        return sum(reach[o] + 1 for o in range(slot)) + w

    def send(src, sem, slot, owner_z, owner_x, h, kind, device):
        return pltpu.make_async_remote_copy(
            src_ref=src, dst_ref=piece(slot, owner_z, owner_x, h), send_sem=sem,
            recv_sem=recv.at[row(slot, owner_z), kind],
            device_id=device, device_id_type=MESH)

    def arrived(slot, w, kind):
        size = SPAN * 2 if kind == LATE else half
        there = held.at[slot, pl.ds(0, size)]
        pltpu.make_async_remote_copy(
            src_ref=there, dst_ref=there, send_sem=up_sem.at[row(slot, w)],
            recv_sem=recv.at[row(slot, w), kind], device_id=right, device_id_type=MESH).wait_recv()

    def sent(slot, sem, pieces):
        there = held.at[slot, pl.ds(0, pieces * half)]
        pltpu.make_async_remote_copy(
            src_ref=there, dst_ref=there, send_sem=sem, recv_sem=recv.at[0, 0],
            device_id=right, device_id_type=MESH).wait_send()

    def goes_up(slot, d):
        climb = 3 if slot == 0 else NZ
        return (z + 1 <= reach[slot]) & (d <= climb)

    columns_of = (x, x_left, x_far, x_right)

    def whole(d):
        return (d == z) & ((z <= 2) | (z >= 6))

    def relay(c, h, kind):
        src = piece(0, 0, columns_of[c], h)

        @pl.when(z < (3 if c == 0 else 2))
        def _():
            send(src, once_sem.at[RELAY_UP], 0, 0, columns_of[c], h, kind, above).start()

        @pl.when((z == 0) | (z >= (6 if c == 0 else 7)))
        def _():
            send(src, once_sem.at[RELAY_DOWN], 0, 0, columns_of[c], h, kind, below).start()

    def plain(slot, d):
        return jnp.logical_not(whole(d)) if slot == 0 else z >= 0

    def onward(slot, d):
        if slot > 0:
            return goes_up(slot, d), z < 0
        chained = jnp.logical_not(whole(d))
        return chained & goes_up(slot, d), chained & (d >= 6)

    def along(slot, d, h):
        w = z - d
        src = piece(slot, w, x, h)
        up, down = onward(slot, d)

        @pl.when(up)
        def _():
            send(src, up_sem.at[row(slot, w)], slot, w, x, h, COLUMN + h, above).start()

        if slot == 0:
            @pl.when(down)
            def _():
                send(src, up_sem.at[row(slot, w)], slot, w, x, h, COLUMN + h, below).start()

            @pl.when(whole(d))
            def _():
                relay(0, h, COLUMN + h)

        @pl.when(plain(slot, d) | (z == 0))
        def _():
            sem = beside_sem.at[row(slot, w)]
            send(src, sem, slot, w, x, h, LEFT if h == 0 else LATE, right).start()
            send(src, sem, slot, w, x, h, LATE if h == 0 else RIGHT, left).start()

    def to_top(h):
        return send(mine(0, h), once_sem.at[TO_TOP], 0, z, x, h, COLUMN + h, top)

    def each(body, slots=range(SEQS)):
        for slot in slots:
            @pl.when(z <= reach[slot])
            def _(slot=slot):
                body(slot)

    def distance(t):
        return t % 2 * ((t + 1) // 2) + (1 - t % 2) * ((NZ - t // 2) % NZ)

    def around(t, slots=range(SEQS)):
        d = distance(t)
        w = z - d

        def passing(slot):
            sem = beside_sem.at[row(slot, w)]
            send(piece(slot, w, x_left, 0), sem, slot, w, x_left, 0, LATE, right).start()
            send(piece(slot, w, x_right, 1), sem, slot, w, x_right, 1, LATE, left).start()

        def body(slot):
            arrived(slot, w, LEFT)
            arrived(slot, w, RIGHT)
            if slot == 0:
                @pl.when(plain(slot, d) | (z == 0))
                def _():
                    passing(slot)

                @pl.when(whole(d))
                def _():
                    relay(1, 0, LEFT)
                    relay(3, 1, RIGHT)
            else:
                passing(slot)

        each(body, slots)

    def tail(t):
        d = distance(t)
        late = ((1, 1), (3, 0), (2, 0), (2, 1))

        @pl.when(whole(d) & (z <= reach[0]))
        def _():
            arrived(0, 0, LATE)
            for c, h in late:
                relay(c, h, LATE)

    def column(t):
        d = distance(t)

        def body(slot):
            for h in range(2):
                arrived(slot, z - d, COLUMN + h)
                along(slot, d, h)

        each(body)

    def settle(t):
        d = distance(t)
        w = z - d

        def body(slot):
            if slot == 0:
                @pl.when(plain(slot, d))
                def _():
                    arrived(slot, w, LATE)
            else:
                arrived(slot, w, LATE)
            store(slot, w).start()

        each(body)

    def finish(t):
        d = distance(t)
        w = z - d

        def body(slot):
            up, down = onward(slot, d)

            @pl.when(up | down)
            def _():
                sent(slot, up_sem.at[row(slot, w)], 2)

            @pl.when(plain(slot, d) | (z == 0))
            def _():
                sent(slot, beside_sem.at[row(slot, w)], 6)

            store(slot, w).wait()

        each(body)

    def column_copy(d):
        peer = (tp + d) % NTP
        first = pl.multiple_of(peer * SPAN, SPAN)
        return pltpu.make_async_remote_copy(
            src_ref=out_w.at[:, pl.ds(first, SPAN)], dst_ref=columns.at[tp],
            send_sem=once_sem.at[W_SEND], recv_sem=once_sem.at[W_RECV],
            device_id={"tp": peer}, device_id_type=MESH)

    def begin(slot):
        for h in range(2):
            along(slot, 0, h)

    @pl.when(low)
    def _():
        for h in range(2):
            to_top(h).start()

    each(begin, (0, 1))

    around(0, (0,))
    each(begin, (2, 3))
    for d in range(1, NTP):
        column_copy(d).start()

    load_q.wait()

    @pl.loop(1, NZ)
    def _(t):
        @pl.when(distance(t) <= z)
        def _():
            column(t)

        @pl.when(t <= SEQS)
        def _():
            q_out[t - 1] = jnp.dot(
                rows_in[t - 1], q_weights[...], preferred_element_type=jnp.float32).astype(jnp.bfloat16)

        @pl.when(t == SEQS + 1)
        def _():
            make_plan(kv, lengths, chosen, plan, named, packed)

    tail(0)
    around(0, (1, 2, 3))

    @pl.loop(1, NZ)
    def _(t):
        @pl.when(distance(t) <= z)
        def _():
            around(t)
            tail(t)

    @pl.loop(0, NZ)
    def _(t):
        @pl.when(distance(t) <= z)
        def _():
            settle(t)

    @pl.loop(0, NZ)
    def _(t):
        @pl.when(distance(t) <= z)
        def _():
            finish(t)

    @pl.when(low)
    def _():
        sent(0, once_sem.at[TO_TOP], 2)

    climbs = z <= reach[0]

    @pl.when(climbs & (z < 2))
    def _():
        sent(0, once_sem.at[RELAY_UP], 8)

    @pl.when(climbs & (z == 2))
    def _():
        sent(0, once_sem.at[RELAY_UP], 2)

    @pl.when(climbs & ((z == 0) | (z == 7)))
    def _():
        sent(0, once_sem.at[RELAY_DOWN], 8)

    @pl.when(climbs & (z == 6))
    def _():
        sent(0, once_sem.at[RELAY_DOWN], 2)

    others = columns.at[pl.ds(0, NTP - 1)]
    pltpu.make_async_remote_copy(
        src_ref=others, dst_ref=others, send_sem=once_sem.at[W_SEND], recv_sem=once_sem.at[W_RECV],
        device_id=right, device_id_type=MESH).wait()


def spread(reach, lengths, chosen, inputs, query_weight, key_weight, value_weight, out_weight):
    dma = pltpu.SemaphoreType.DMA
    named = SEQS * (SPAN // KB)
    rows = sum(r + 1 for r in reach)
    return pl.pallas_call(
        lambda *refs: spread_kernel(reach, *refs),
        name="spread",
        out_shape=(
            jax.ShapeDtypeStruct((SEQS, NZ * NX * SPAN, 2 * HD), jnp.bfloat16),
            jax.ShapeDtypeStruct((NTP, SPAN, SPAN), jnp.bfloat16),
            jax.ShapeDtypeStruct((SEQS, SPAN, 2 * HD), jnp.bfloat16),
            jax.ShapeDtypeStruct((MORE + named, LANES), jnp.int32),
        ),
        in_specs=[SMEM, VMEM] + [ANY] * 5,
        out_specs=(ANY, ANY, VMEM, VMEM),
        scratch_shapes=[
            pltpu.VMEM((SEQS, NZ * NX * SPAN, 2 * HD), jnp.bfloat16),
            pltpu.VMEM((SEQS, SPAN, MODEL), jnp.bfloat16),
            pltpu.VMEM((MODEL, 2 * HD), jnp.bfloat16),
            pltpu.VMEM((MODEL, 2 * HD), jnp.bfloat16),
            pltpu.VMEM((SEQS, SPAN, 2 * HD), jnp.bfloat16),
            pltpu.VMEM((named, LANES), jnp.int32),
            pltpu.VMEM((MORE, LANES), jnp.int32),
            dma((SEQS + 3,)),
            dma((rows,)),
            dma((rows, 5)),
            dma((rows,)),
            dma((rows,)),
            dma((5,)),
        ],
        compiler_params=pltpu.CompilerParams(
            collective_id=0 if reach == REACH else 1, has_side_effects=True
        ),
    )(lengths, chosen, inputs, query_weight, key_weight, value_weight, out_weight)


def attend_kernel(lengths, plan, q_in, cache, out, q, keys, scores, high, total, acc, q_sem, own_sems, sems):
    kv = lax.axis_index("kv")
    slots = plan[MORE, LIVE]
    blocks = SPAN // KB
    heads = 2

    def sequence(slot):
        b = plan[MORE, ORDER + slot]
        return b, plan[b, COUNT]

    def own_copy(slot):
        span = pl.ds(pl.multiple_of(kv * SPAN, SPAN), SPAN)
        return pltpu.make_async_copy(
            cache.at[slot, span], keys.at[slot % 2, pl.ds(0, SPAN)], own_sems.at[slot % 2])

    def block_copy(slot, block, e):
        row = pl.multiple_of(block * KB, KB)
        to = pl.multiple_of(SPAN + e * KB, KB)
        return pltpu.make_async_copy(
            cache.at[slot, pl.ds(row, KB)], keys.at[slot % 2, pl.ds(to, KB)], sems.at[slot % 2])

    def fetch(slot):
        b, n = sequence(slot)
        own_copy(slot).start()

        @pl.loop(0, n)
        def _(e):
            block_copy(slot, plan[b, e] % 256, e).start()

        past = pl.ds(pl.multiple_of(SPAN + n * KB, KB), 3 * KB)
        keys[slot % 2, past, :] = jnp.zeros((3 * KB, 2 * HD), jnp.bfloat16)

    def chunk_start(c):
        return c * CHUNK if isinstance(c, int) else pl.multiple_of(c * CHUNK, CHUNK)

    def part(h, i):
        return slice(h * SPAN + i * KB, h * SPAN + (i + 1) * KB)

    def compute(slot):
        b, n = sequence(slot)
        chunks = 1 + (n + 3) // 4
        for few in (1, 2):
            pl.when(chunks == few)(lambda few=few: compute_chunks(slot, b, n, few))
        pl.when(chunks > 2)(lambda: compute_chunks(slot, b, n, chunks))

    def compute_chunks(slot, b, n, chunks):
        held = keys.at[slot % 2]

        def each_chunk(first):
            def run(body):
                if isinstance(chunks, int):
                    for c in range(first, chunks):
                        body(c)
                else:
                    pl.loop(first, chunks)(body)
            return run

        own_copy(slot).wait()
        both = q[b]
        stacked = jnp.concatenate([both[:, :HD], both[:, HD:]], axis=0)
        lane = lax.broadcasted_iota(jnp.int32, (1, CHUNK), 1)
        place = lane // KB

        def score(first):
            return lax.dot_general(stacked, held[pl.ds(first, CHUNK), :HD], (((1,), (1,)), ((), ())),
                                   preferred_element_type=jnp.float32) * (HD ** -0.5)

        s = score(0)
        col = lax.broadcasted_iota(jnp.int32, (KB, CHUNK), 1)
        row = lax.broadcasted_iota(jnp.int32, (KB, CHUNK), 0)
        for i in range(blocks):
            bits = plan[MORE + b * 4 + i, LOCAL] | (1 << i)
            named = jnp.zeros((1, CHUNK), jnp.int32)
            for p in range(blocks):
                named = jnp.where(place == p, (bits >> p) & 1, named)
            limit = jnp.where(named != 0, lane, SPAN)
            for h in range(heads):
                now = jnp.where(limit <= row + i * KB, s[part(h, i)], -jnp.inf)
                scores[0, part(h, i), :] = now
                high[part(h, i), :] = jnp.maximum(now[:, :HD], now[:, HD:])

        @pl.loop(0, n)
        def _(e):
            block_copy(slot, 0, e).wait()

        @each_chunk(1)
        def _(c):
            s = score(chunk_start(c))
            codes = []
            for p in range(blocks):
                e = (c - 1) * 4 + p
                codes.append(jnp.where(e < n, plan[b, e] // 256, 0))
            for i in range(blocks):
                shift = jnp.zeros((1, CHUNK), jnp.float32)
                for p in range(blocks):
                    absent = jnp.where((codes[p] >> i) & 1 != 0, jnp.float32(0), -jnp.inf)
                    shift = jnp.where(place == p, absent, shift)
                for h in range(heads):
                    now = s[part(h, i)] + shift
                    scores[c, part(h, i), :] = now
                    high[part(h, i), :] = jnp.maximum(high[part(h, i), :], jnp.maximum(now[:, :HD], now[:, HD:]))

        for h in range(heads):
            for i in range(blocks):
                top = jnp.max(high[part(h, i), :], axis=1, keepdims=True)
                high[part(h, i), :] = jnp.broadcast_to(top, (KB, HD))
        total[...] = jnp.zeros_like(total)

        @each_chunk(0)
        def _(c):
            for h in range(heads):
                for i in range(blocks):
                    top = high[part(h, i), :]
                    left = jnp.exp(scores[c, part(h, i), :HD] - top)
                    right = jnp.exp(scores[c, part(h, i), HD:] - top)
                    scores[c, part(h, i), :HD] = left
                    scores[c, part(h, i), HD:] = right
                    total[part(h, i), :] += left + right

        again = jnp.int32(0)
        for i in range(blocks):
            again += plan[MORE + b * 4 + i, REPEATS]

        def self_part(h, i):
            return jnp.where(col == row + i * KB, scores[0, part(h, i), :], 0.0)

        @pl.when(again > 0)
        def _():
            for h in range(heads):
                for i in range(blocks):
                    e = self_part(h, i)
                    times = plan[MORE + b * 4 + i, REPEATS].astype(jnp.float32)
                    total[part(h, i), :] += times * (e[:, :HD] + e[:, HD:])

        for h in range(heads):
            for i in range(blocks):
                share = 1.0 / jnp.sum(total[part(h, i), :], axis=1, keepdims=True)
                total[part(h, i), :] = jnp.broadcast_to(share, (KB, HD))
        acc[...] = jnp.zeros_like(acc)

        @pl.when(again > 0)
        def _():
            for h in range(heads):
                for i in range(blocks):
                    share = total[part(h, i), :]
                    e = self_part(h, i)
                    weight = jnp.concatenate([e[:, :HD] * share, e[:, HD:] * share], axis=1)
                    times = plan[MORE + b * 4 + i, REPEATS].astype(jnp.float32)
                    acc[part(h, i), :] = times * jnp.dot(
                        weight.astype(jnp.bfloat16), held[:SPAN, HD:], preferred_element_type=jnp.float32)

        @each_chunk(0)
        def _(c):
            share = total[...]
            weight = jnp.concatenate([scores[c, :, :HD] * share, scores[c, :, HD:] * share], axis=1)
            acc[...] += jnp.dot(weight.astype(jnp.bfloat16),
                                held[pl.ds(chunk_start(c), CHUNK), HD:],
                                preferred_element_type=jnp.float32)

        pos = kv * SPAN + lax.broadcasted_iota(jnp.int32, (SPAN, HD), 0)
        for h in range(heads):
            done = jnp.where(pos < lengths[b], acc[h * SPAN:(h + 1) * SPAN, :], 0.0)
            out[slot, :, h * HD:(h + 1) * HD] = done.astype(jnp.bfloat16)

    load_q = pltpu.make_async_copy(q_in, q, q_sem)
    load_q.start()

    @pl.when(slots > 0)
    def _():
        fetch(jnp.int32(0))

    @pl.loop(slots, SEQS)
    def _(slot):
        out[slot] = jnp.zeros((SPAN, 2 * HD), jnp.bfloat16)

    load_q.wait()

    @pl.loop(0, slots)
    def _(slot):
        @pl.when(slot + 1 < slots)
        def _():
            fetch(slot + 1)

        compute(slot)


def attend(lengths, plan, q, cache):
    most = NZ * NX * (SPAN // KB)
    rows = 2 * SPAN
    return pl.pallas_call(
        attend_kernel,
        name="attend",
        out_shape=jax.ShapeDtypeStruct((SEQS, SPAN, 2 * HD), jnp.bfloat16),
        in_specs=[SMEM, SMEM, ANY, ANY],
        out_specs=VMEM,
        scratch_shapes=[
            pltpu.VMEM((SEQS, SPAN, 2 * HD), jnp.bfloat16),
            pltpu.VMEM((2, SPAN + most * KB, 2 * HD), jnp.bfloat16),
            pltpu.VMEM((1 + most // 4, rows, CHUNK), jnp.float32),
            pltpu.VMEM((rows, HD), jnp.float32),
            pltpu.VMEM((rows, HD), jnp.float32),
            pltpu.VMEM((rows, HD), jnp.float32),
            pltpu.SemaphoreType.DMA,
            pltpu.SemaphoreType.DMA((2,)),
            pltpu.SemaphoreType.DMA((2,)),
        ],
    )(lengths, plan, q, cache)


def mix_kernel(reach, lengths, attended, columns_in, out_w, out, groups, own, columns, own_w, acc,
               load_sem, next_recv, prev_recv, core_recv, sent):
    kv, tp = lax.axis_index("kv"), lax.axis_index("tp")
    z = kv // NX
    y, core = tp // 2, tp % 2
    y_next, y_prev, y_far = (y + 1) % NY, (y + NY - 1) % NY, (y + 2) % NY
    after, before = {"tp": y_next * 2 + core}, {"tp": y_prev * 2 + core}
    partner = {"tp": y * 2 + 1 - core}
    half = SPAN // 2

    barrier = pltpu.get_barrier_semaphore()
    for d in (after, before, partner):
        pl.semaphore_signal(barrier, inc=1, device_id=d, device_id_type=MESH)
    my_columns = out_w.at[:, pl.ds(pl.multiple_of(tp * SPAN, SPAN), SPAN)]
    loads = (
        pltpu.make_async_copy(attended, own, load_sem.at[0]),
        pltpu.make_async_copy(my_columns, own_w, load_sem.at[1]),
        pltpu.make_async_copy(columns_in, columns, load_sem.at[2]),
    )
    for load in loads:
        load.start()
    loads[0].wait()
    pl.semaphore_wait(barrier, 3)

    def piece(owner_y, owner_core, slot, h):
        return groups.at[owner_y * 2 + owner_core, slot, pl.ds(h * half, half)]

    def copy(src, dst, send_sem, recv_sem, device):
        return pltpu.make_async_remote_copy(
            src_ref=src, dst_ref=dst, send_sem=send_sem, recv_sem=recv_sem,
            device_id=device, device_id_type=MESH)

    def mine(slot, h):
        return own.at[slot, pl.ds(h * half, half)]

    def to_next(slot, h):
        return copy(mine(slot, h), piece(y, core, slot, h), sent.at[slot], next_recv.at[h, slot], after)

    def to_prev(slot, h):
        return copy(mine(slot, h), piece(y, core, slot, h), sent.at[slot], prev_recv.at[h, slot], before)

    def on_next(slot):
        here = piece(y_prev, core, slot, 0)
        return copy(here, here, sent.at[slot], next_recv.at[2, slot], after)

    def on_prev(slot):
        here = piece(y_next, core, slot, 1)
        return copy(here, here, sent.at[slot], prev_recv.at[2, slot], before)

    def across(stage, owner_y, slot, h, src=None):
        here = piece(owner_y, core, slot, h)
        return copy(here if src is None else src, here, sent.at[slot], core_recv.at[stage, slot], partner)

    def crossed(stage, slot):
        both = groups.at[0, slot]
        copy(both, both, sent.at[slot], core_recv.at[stage, slot], partner).wait_recv()

    def each(body):
        for slot in range(SEQS):
            @pl.when(z <= reach[slot])
            def _(slot=slot):
                body(slot)

    def product(rows, weight):
        part = jnp.dot(rows, weight, preferred_element_type=jnp.float32)
        return part.astype(jnp.bfloat16).astype(jnp.float32)

    def add(slot, owner_y, owner_core):
        g = owner_y * 2 + owner_core
        acc[slot] += product(groups[g, slot], columns[g])

    def begin(slot):
        to_next(slot, 0).start()
        to_prev(slot, 1).start()
        to_next(slot, 1).start()
        to_prev(slot, 0).start()
        for h in range(2):
            across(0, y, slot, h, mine(slot, h)).start()

    def first(slot):
        acc[slot] = product(own[slot], own_w[...])

    def relay(slot):
        to_next(slot, 0).wait_recv()
        on_next(slot).start()
        across(1, y_prev, slot, 0).start()
        to_prev(slot, 1).wait_recv()
        on_prev(slot).start()
        across(2, y_next, slot, 1).start()
        to_next(slot, 1).wait_recv()
        across(1, y_prev, slot, 1).start()
        to_prev(slot, 0).wait_recv()
        across(2, y_next, slot, 0).start()

    def near(slot):
        crossed(0, slot)
        for owner_y, owner_core in ((y, 1 - core), (y_prev, core), (y_next, core)):
            add(slot, owner_y, owner_core)

    def middle(slot):
        for stage, owner_y in ((1, y_prev), (2, y_next)):
            crossed(stage, slot)
            add(slot, owner_y, 1 - core)

    def far(slot):
        on_next(slot).wait_recv()
        across(3, y_far, slot, 0).start()
        on_prev(slot).wait_recv()
        across(3, y_far, slot, 1).start()
        if slot > 0:
            last(slot - 1)
        add(slot, y_far, core)

    def last(slot):
        crossed(3, slot)
        add(slot, y_far, 1 - core)

    def finish(slot):
        all_sent = groups.at[pl.ds(0, 7), slot]
        copy(all_sent, all_sent, sent.at[slot], core_recv.at[0, slot], partner).wait_send()

    each(begin)
    acc[...] = jnp.zeros_like(acc)
    loads[1].wait()
    each(first)
    loads[2].wait()

    def both(slot):
        relay(slot)
        near(slot)

    each(both)
    each(middle)
    each(far)
    for slot in range(SEQS):
        beyond = z <= reach[slot + 1] if slot + 1 < SEQS else z < 0

        @pl.when((z <= reach[slot]) & jnp.logical_not(beyond))
        def _(slot=slot):
            last(slot)

    for b in range(SEQS):
        slot = jnp.int32(0)
        for o in range(SEQS):
            if o < b:
                slot += (lengths[o] >= lengths[b]).astype(jnp.int32)
            elif o > b:
                slot += (lengths[o] > lengths[b]).astype(jnp.int32)
        out[b] = acc[slot].astype(jnp.bfloat16)
    each(finish)


def mix(reach, lengths, own, columns, out_weight):
    dma = pltpu.SemaphoreType.DMA
    return pl.pallas_call(
        lambda *refs: mix_kernel(reach, *refs),
        name="mix",
        out_shape=jax.ShapeDtypeStruct((SEQS, SPAN, SPAN), jnp.bfloat16),
        in_specs=[SMEM, ANY, ANY, ANY],
        out_specs=VMEM,
        scratch_shapes=[
            pltpu.VMEM((NTP, SEQS, SPAN, 2 * HD), jnp.bfloat16),
            pltpu.VMEM((SEQS, SPAN, 2 * HD), jnp.bfloat16),
            pltpu.VMEM((NTP, SPAN, SPAN), jnp.bfloat16),
            pltpu.VMEM((SPAN, SPAN), jnp.bfloat16),
            pltpu.VMEM((SEQS, SPAN, SPAN), jnp.float32),
            dma((3,)),
            dma((3, SEQS)),
            dma((3, SEQS)),
            dma((4, SEQS)),
            dma((SEQS,)),
        ],
        compiler_params=pltpu.CompilerParams(
            collective_id=2 if reach == REACH else 3, has_side_effects=True
        ),
    )(lengths, own, columns, out_weight)


def shards(inputs, query_weight, key_weight, value_weight, out_weight, chosen, lengths):
    def rest(reach):
        cache, columns, queries, plan = spread(
            reach, lengths, chosen, inputs, query_weight, key_weight, value_weight, out_weight)
        attended = attend(lengths, plan, queries, cache)
        return mix(reach, lengths, attended, columns, out_weight)

    score = jnp.where(lengths > 3072, 6, jnp.where(lengths > 2048, 3, jnp.where(lengths > 1024, 2, 0)))
    near = jnp.sum(score) < 12
    return lax.cond(near, lambda: rest(NEAR_REACH), lambda: rest(REACH))


def solution(mesh):
    placed = (
        P(None, "kv", None),
        P(None, "tp"),
        P(None, "tp"),
        P(None, "tp"),
        P("tp", None),
        P(None, "kv", None),
        P(),
    )
    return jax.shard_map(
        shards, mesh=mesh, in_specs=placed, out_specs=P(None, "kv", "tp"), check_vma=False
    )
```

```python
import jax
import jax.numpy as jnp
from jax import lax
from jax.experimental import pallas as pl
from jax.experimental.pallas import tpu as pltpu
from jax.sharding import PartitionSpec as P

HD = 128
KB = 64
TOPK = 32
SEQS = 4
SPAN = 256
MODEL = 2048
NZ, NX, NY = 8, 4, 4
NTP = 8
REACH = (7, 5, 3, 2)
NEAR_REACH = (7, 2, 1, 0)
LANES = 128
MORE = 8
COUNT = 124
REPEATS, LOCAL, LIVE, ORDER = 0, 1, 2, 3
CHUNK = 256
MESH = pl.DeviceIdType.MESH
ANY = pl.BlockSpec(memory_space=pl.ANY)
SMEM = pl.BlockSpec(memory_space=pltpu.SMEM)
VMEM = pl.BlockSpec(memory_space=pltpu.VMEM)


def sequence_of(slot, lengths):
    size = [lengths[b] for b in range(SEQS)]
    found = jnp.int32(0)
    for b in range(SEQS):
        rank = jnp.int32(0)
        for o in range(SEQS):
            if o < b:
                rank += (size[o] >= size[b]).astype(jnp.int32)
            elif o > b:
                rank += (size[o] > size[b]).astype(jnp.int32)
        found += jnp.where(rank == slot, b, 0)
    return found


def make_plan(kv, lengths, chosen, plan, named, packed):
    named[...] = jnp.full(named.shape, -1, jnp.int32)
    for b in range(SEQS):
        named[b * 4:(b + 1) * 4, :TOPK] = chosen[b]
    block = named[...]
    lane = lax.broadcasted_iota(jnp.int32, block.shape, 1)
    row = lax.broadcasted_iota(jnp.int32, block.shape, 0)
    i = row % 4
    length = jnp.full(block.shape, lengths[0])
    for b in range(1, SEQS):
        length = jnp.where(row // 4 == b, lengths[b], length)
    member = jnp.zeros(block.shape, jnp.int32)
    for e in range(TOPK):
        member |= (block[:, e:e + 1] == lane).astype(jnp.int32)
    member = jnp.where((kv * 4 + i) * KB < length, member, 0)
    repeats = jnp.sum((block == kv * 4 + i).astype(jnp.int32), axis=1, keepdims=True) - 1
    here = lane - kv * 4
    inside = (here >= 0) & (here < 4)
    local = jnp.sum(jnp.where(inside, member << jnp.where(inside, here, 0), 0), axis=1, keepdims=True)
    named[...] = jnp.where(here < 0, member << i, 0)
    live = jnp.int32(0)
    for b in range(SEQS):
        live += (lengths[b] > kv * SPAN).astype(jnp.int32)
    more = jnp.where(lane == REPEATS, repeats, jnp.where(lane == LOCAL, local, live))
    for j in range(SEQS):
        more = jnp.where(lane == ORDER + j, sequence_of(j, lengths), more)
    plan[MORE:, :] = more

    packed[...] = jnp.zeros(packed.shape, jnp.int32)
    for b in range(SEQS):
        packed[b:b + 1, :] = jnp.sum(named[b * 4:(b + 1) * 4, :], axis=0, keepdims=True)
    code = packed[...]
    lane = lax.broadcasted_iota(jnp.int32, code.shape, 1)
    held = (code != 0).astype(jnp.int32)
    code = lane + 256 * code
    steps = (1, 2, 4, 8, 16, 32, 64)
    upto = held
    for s in steps:
        upto += jnp.where(lane >= s, pltpu.roll(upto, s, 1), 0)
    count = jnp.sum(held, axis=1, keepdims=True)
    gap = lane - (upto - 1)
    for s in steps:
        there = pltpu.roll(code, LANES - s, 1)
        there_gap = pltpu.roll(gap, LANES - s, 1)
        take = (pltpu.roll(held, LANES - s, 1) != 0) & ((there_gap & s) != 0)
        stay = (held != 0) & ((gap & s) == 0)
        code = jnp.where(take, there, code)
        gap = jnp.where(take, there_gap, gap)
        held = (take | stay).astype(jnp.int32)
    plan[:MORE, :] = jnp.where(lane == COUNT, count, code)


def spread_kernel(reach, lengths, chosen, inputs, query_w, key_w, value_w, out_w,
                  cache, columns, q_out, plan, held, rows_in, q_weights, kv_weights, projected,
                  named, packed, load_sem, store_sem, recv, up_sem, beside_sem, once_sem):
    kv, tp = lax.axis_index("kv"), lax.axis_index("tp")
    z, x = kv // NX, kv % NX
    right = {"kv": z * NX + (x + 1) % NX}
    left = {"kv": z * NX + (x + NX - 1) % NX}
    x_right, x_left, x_far = (x + 1) % NX, (x + NX - 1) % NX, (x + 2) % NX
    half = SPAN // 2
    TO_TOP, RELAY_UP, RELAY_DOWN, W_SEND, W_RECV = range(5)
    COLUMN, LEFT, RIGHT, LATE = 0, 2, 3, 4

    loads = [
        pltpu.make_async_copy(key_w, kv_weights.at[:, pl.ds(0, HD)], load_sem.at[0]),
        pltpu.make_async_copy(value_w, kv_weights.at[:, pl.ds(HD, HD)], load_sem.at[1]),
    ]
    loads += [pltpu.make_async_copy(inputs.at[b], rows_in.at[b], load_sem.at[2 + b]) for b in range(SEQS)]
    load_q = pltpu.make_async_copy(query_w, q_weights, load_sem.at[2 + SEQS])
    for load in loads:
        load.start()

    above = {"kv": (z + 1) % NZ * NX + x}
    below = {"kv": (z + NZ - 1) % NZ * NX + x}
    top = {"kv": (NZ - 1) * NX + x}

    barrier = pltpu.get_barrier_semaphore()

    def greet(device):
        pl.semaphore_signal(barrier, inc=1, device_id=device, device_id_type=MESH)

    for d in (above, below, right, left):
        greet(d)
    for d in range(1, NTP):
        greet({"tp": (tp + d) % NTP})
    low = (z >= 1) & (z <= 2)

    @pl.when(low)
    def _():
        greet(top)

    @pl.when(z == NZ - 1)
    def _():
        for w in (1, 2):
            greet({"kv": w * NX + x})

    loads[0].wait()
    loads[1].wait()
    for b in range(SEQS):
        loads[2 + b].wait()
        projected[b] = jnp.dot(rows_in[b], kv_weights[...], preferred_element_type=jnp.float32).astype(jnp.bfloat16)
    load_q.start()
    for slot in range(SEQS):
        held[slot, pl.ds(pl.multiple_of(kv * SPAN, SPAN), SPAN), :] = projected[sequence_of(slot, lengths)]

    pl.semaphore_wait(barrier, 4 + NTP - 1 + low.astype(jnp.int32) + z // (NZ - 1) * 2)

    def piece(slot, owner_z, owner_x, h):
        first = pl.multiple_of((owner_z * NX + owner_x) * SPAN + h * half, half)
        return held.at[slot, pl.ds(first, half)]

    def mine(slot, h):
        return piece(slot, z, x, h)

    def store(slot, w):
        span = pl.ds(pl.multiple_of(w * NX * SPAN, NX * SPAN), NX * SPAN)
        return pltpu.make_async_copy(held.at[slot, span], cache.at[slot, span], store_sem.at[row(slot, w)])

    def row(slot, w):
        return sum(reach[o] + 1 for o in range(slot)) + w

    def send(src, sem, slot, owner_z, owner_x, h, kind, device):
        return pltpu.make_async_remote_copy(
            src_ref=src, dst_ref=piece(slot, owner_z, owner_x, h), send_sem=sem,
            recv_sem=recv.at[row(slot, owner_z), kind],
            device_id=device, device_id_type=MESH)

    def arrived(slot, w, kind):
        size = SPAN * 2 if kind == LATE else half
        there = held.at[slot, pl.ds(0, size)]
        pltpu.make_async_remote_copy(
            src_ref=there, dst_ref=there, send_sem=up_sem.at[row(slot, w)],
            recv_sem=recv.at[row(slot, w), kind], device_id=right, device_id_type=MESH).wait_recv()

    def sent(slot, sem, pieces):
        there = held.at[slot, pl.ds(0, pieces * half)]
        pltpu.make_async_remote_copy(
            src_ref=there, dst_ref=there, send_sem=sem, recv_sem=recv.at[0, 0],
            device_id=right, device_id_type=MESH).wait_send()

    def goes_up(slot, d):
        climb = 3 if slot == 0 else NZ
        return (z + 1 <= reach[slot]) & (d <= climb)

    columns_of = (x, x_left, x_far, x_right)

    def whole(d):
        return (d == z) & ((z <= 2) | (z >= 6))

    def relay(c, h, kind):
        src = piece(0, 0, columns_of[c], h)

        @pl.when(z < (3 if c == 0 else 2))
        def _():
            send(src, once_sem.at[RELAY_UP], 0, 0, columns_of[c], h, kind, above).start()

        @pl.when((z == 0) | (z >= (6 if c == 0 else 7)))
        def _():
            send(src, once_sem.at[RELAY_DOWN], 0, 0, columns_of[c], h, kind, below).start()

    def plain(slot, d):
        return jnp.logical_not(whole(d)) if slot == 0 else z >= 0

    def onward(slot, d):
        if slot > 0:
            return goes_up(slot, d), z < 0
        chained = jnp.logical_not(whole(d))
        return chained & goes_up(slot, d), chained & (d >= 6)

    def along(slot, d, h):
        w = z - d
        src = piece(slot, w, x, h)
        up, down = onward(slot, d)

        @pl.when(up)
        def _():
            send(src, up_sem.at[row(slot, w)], slot, w, x, h, COLUMN + h, above).start()

        if slot == 0:
            @pl.when(down)
            def _():
                send(src, up_sem.at[row(slot, w)], slot, w, x, h, COLUMN + h, below).start()

            @pl.when(whole(d))
            def _():
                relay(0, h, COLUMN + h)

        @pl.when(plain(slot, d) | (z == 0))
        def _():
            sem = beside_sem.at[row(slot, w)]
            send(src, sem, slot, w, x, h, LEFT if h == 0 else LATE, right).start()
            send(src, sem, slot, w, x, h, LATE if h == 0 else RIGHT, left).start()

    def to_top(h):
        return send(mine(0, h), once_sem.at[TO_TOP], 0, z, x, h, COLUMN + h, top)

    def each(body, slots=range(SEQS)):
        for slot in slots:
            @pl.when(z <= reach[slot])
            def _(slot=slot):
                body(slot)

    def distance(t):
        return t % 2 * ((t + 1) // 2) + (1 - t % 2) * ((NZ - t // 2) % NZ)

    def around(t, slots=range(SEQS)):
        d = distance(t)
        w = z - d

        def passing(slot):
            sem = beside_sem.at[row(slot, w)]
            send(piece(slot, w, x_left, 0), sem, slot, w, x_left, 0, LATE, right).start()
            send(piece(slot, w, x_right, 1), sem, slot, w, x_right, 1, LATE, left).start()

        def body(slot):
            arrived(slot, w, LEFT)
            arrived(slot, w, RIGHT)
            if slot == 0:
                @pl.when(plain(slot, d) | (z == 0))
                def _():
                    passing(slot)

                @pl.when(whole(d))
                def _():
                    relay(1, 0, LEFT)
                    relay(3, 1, RIGHT)
            else:
                passing(slot)

        each(body, slots)

    def tail(t):
        d = distance(t)
        late = ((1, 1), (3, 0), (2, 0), (2, 1))

        @pl.when(whole(d) & (z <= reach[0]))
        def _():
            arrived(0, 0, LATE)
            for c, h in late:
                relay(c, h, LATE)

    def column(t):
        d = distance(t)

        def body(slot):
            for h in range(2):
                arrived(slot, z - d, COLUMN + h)
                along(slot, d, h)

        each(body)

    def settle(t):
        d = distance(t)
        w = z - d

        def body(slot):
            if slot == 0:
                @pl.when(plain(slot, d))
                def _():
                    arrived(slot, w, LATE)
            else:
                arrived(slot, w, LATE)
            store(slot, w).start()

        each(body)

    def finish(t):
        d = distance(t)
        w = z - d

        def body(slot):
            up, down = onward(slot, d)

            @pl.when(up | down)
            def _():
                sent(slot, up_sem.at[row(slot, w)], 2)

            @pl.when(plain(slot, d) | (z == 0))
            def _():
                sent(slot, beside_sem.at[row(slot, w)], 6)

            store(slot, w).wait()

        each(body)

    def column_copy(d):
        peer = (tp + d) % NTP
        first = pl.multiple_of(peer * SPAN, SPAN)
        return pltpu.make_async_remote_copy(
            src_ref=out_w.at[:, pl.ds(first, SPAN)], dst_ref=columns.at[tp],
            send_sem=once_sem.at[W_SEND], recv_sem=once_sem.at[W_RECV],
            device_id={"tp": peer}, device_id_type=MESH)

    def begin(slot):
        for h in range(2):
            along(slot, 0, h)

    @pl.when(low)
    def _():
        for h in range(2):
            to_top(h).start()

    each(begin, (0, 1))

    around(0, (0,))
    each(begin, (2, 3))
    for d in range(1, NTP):
        column_copy(d).start()

    load_q.wait()

    @pl.loop(1, NZ)
    def _(t):
        @pl.when(distance(t) <= z)
        def _():
            column(t)

        @pl.when(t <= SEQS)
        def _():
            q_out[t - 1] = jnp.dot(
                rows_in[t - 1], q_weights[...], preferred_element_type=jnp.float32).astype(jnp.bfloat16)

        @pl.when(t == SEQS + 1)
        def _():
            make_plan(kv, lengths, chosen, plan, named, packed)

    tail(0)
    around(0, (1, 2, 3))

    @pl.loop(1, NZ)
    def _(t):
        @pl.when(distance(t) <= z)
        def _():
            around(t)
            tail(t)

    @pl.loop(0, NZ)
    def _(t):
        @pl.when(distance(t) <= z)
        def _():
            settle(t)

    @pl.loop(0, NZ)
    def _(t):
        @pl.when(distance(t) <= z)
        def _():
            finish(t)

    @pl.when(low)
    def _():
        sent(0, once_sem.at[TO_TOP], 2)

    climbs = z <= reach[0]

    @pl.when(climbs & (z < 2))
    def _():
        sent(0, once_sem.at[RELAY_UP], 8)

    @pl.when(climbs & (z == 2))
    def _():
        sent(0, once_sem.at[RELAY_UP], 2)

    @pl.when(climbs & ((z == 0) | (z == 7)))
    def _():
        sent(0, once_sem.at[RELAY_DOWN], 8)

    @pl.when(climbs & (z == 6))
    def _():
        sent(0, once_sem.at[RELAY_DOWN], 2)

    others = columns.at[pl.ds(0, NTP - 1)]
    pltpu.make_async_remote_copy(
        src_ref=others, dst_ref=others, send_sem=once_sem.at[W_SEND], recv_sem=once_sem.at[W_RECV],
        device_id=right, device_id_type=MESH).wait()


def spread(reach, lengths, chosen, inputs, query_weight, key_weight, value_weight, out_weight):
    dma = pltpu.SemaphoreType.DMA
    named = SEQS * (SPAN // KB)
    rows = sum(r + 1 for r in reach)
    return pl.pallas_call(
        lambda *refs: spread_kernel(reach, *refs),
        name="spread",
        out_shape=(
            jax.ShapeDtypeStruct((SEQS, NZ * NX * SPAN, 2 * HD), jnp.bfloat16),
            jax.ShapeDtypeStruct((NTP, SPAN, SPAN), jnp.bfloat16),
            jax.ShapeDtypeStruct((SEQS, SPAN, 2 * HD), jnp.bfloat16),
            jax.ShapeDtypeStruct((MORE + named, LANES), jnp.int32),
        ),
        in_specs=[SMEM, VMEM] + [ANY] * 5,
        out_specs=(ANY, ANY, VMEM, VMEM),
        scratch_shapes=[
            pltpu.VMEM((SEQS, NZ * NX * SPAN, 2 * HD), jnp.bfloat16),
            pltpu.VMEM((SEQS, SPAN, MODEL), jnp.bfloat16),
            pltpu.VMEM((MODEL, 2 * HD), jnp.bfloat16),
            pltpu.VMEM((MODEL, 2 * HD), jnp.bfloat16),
            pltpu.VMEM((SEQS, SPAN, 2 * HD), jnp.bfloat16),
            pltpu.VMEM((named, LANES), jnp.int32),
            pltpu.VMEM((MORE, LANES), jnp.int32),
            dma((SEQS + 3,)),
            dma((rows,)),
            dma((rows, 5)),
            dma((rows,)),
            dma((rows,)),
            dma((5,)),
        ],
        compiler_params=pltpu.CompilerParams(
            collective_id=0 if reach == REACH else 1, has_side_effects=True
        ),
    )(lengths, chosen, inputs, query_weight, key_weight, value_weight, out_weight)


def attend_kernel(lengths, plan, q_in, cache, out, q, keys, scores, high, total, acc, q_sem, own_sems, sems):
    kv = lax.axis_index("kv")
    slots = plan[MORE, LIVE]
    blocks = SPAN // KB
    heads = 2

    def sequence(slot):
        b = plan[MORE, ORDER + slot]
        return b, plan[b, COUNT]

    def own_copy(slot):
        span = pl.ds(pl.multiple_of(kv * SPAN, SPAN), SPAN)
        return pltpu.make_async_copy(
            cache.at[slot, span], keys.at[slot % 2, pl.ds(0, SPAN)], own_sems.at[slot % 2])

    def block_copy(slot, block, e):
        row = pl.multiple_of(block * KB, KB)
        to = pl.multiple_of(SPAN + e * KB, KB)
        return pltpu.make_async_copy(
            cache.at[slot, pl.ds(row, KB)], keys.at[slot % 2, pl.ds(to, KB)], sems.at[slot % 2])

    def fetch(slot):
        b, n = sequence(slot)
        own_copy(slot).start()

        @pl.loop(0, n)
        def _(e):
            block_copy(slot, plan[b, e] % 256, e).start()

        past = pl.ds(pl.multiple_of(SPAN + n * KB, KB), 3 * KB)
        keys[slot % 2, past, :] = jnp.zeros((3 * KB, 2 * HD), jnp.bfloat16)

    def chunk_start(c):
        return c * CHUNK if isinstance(c, int) else pl.multiple_of(c * CHUNK, CHUNK)

    def part(h, i):
        return slice(h * SPAN + i * KB, h * SPAN + (i + 1) * KB)

    def compute(slot):
        b, n = sequence(slot)
        chunks = 1 + (n + 3) // 4
        for few in (1, 2):
            pl.when(chunks == few)(lambda few=few: compute_chunks(slot, b, n, few))
        pl.when(chunks > 2)(lambda: compute_chunks(slot, b, n, chunks))

    def compute_chunks(slot, b, n, chunks):
        held = keys.at[slot % 2]

        def each_chunk(first):
            def run(body):
                if isinstance(chunks, int):
                    for c in range(first, chunks):
                        body(c)
                else:
                    pl.loop(first, chunks)(body)
            return run

        own_copy(slot).wait()
        both = q[b]
        stacked = jnp.concatenate([both[:, :HD], both[:, HD:]], axis=0)
        lane = lax.broadcasted_iota(jnp.int32, (1, CHUNK), 1)
        place = lane // KB

        def score(first):
            return lax.dot_general(stacked, held[pl.ds(first, CHUNK), :HD], (((1,), (1,)), ((), ())),
                                   preferred_element_type=jnp.float32) * (HD ** -0.5)

        s = score(0)
        col = lax.broadcasted_iota(jnp.int32, (KB, CHUNK), 1)
        row = lax.broadcasted_iota(jnp.int32, (KB, CHUNK), 0)
        for i in range(blocks):
            bits = plan[MORE + b * 4 + i, LOCAL] | (1 << i)
            named = jnp.zeros((1, CHUNK), jnp.int32)
            for p in range(blocks):
                named = jnp.where(place == p, (bits >> p) & 1, named)
            limit = jnp.where(named != 0, lane, SPAN)
            for h in range(heads):
                now = jnp.where(limit <= row + i * KB, s[part(h, i)], -jnp.inf)
                scores[0, part(h, i), :] = now
                high[part(h, i), :] = jnp.maximum(now[:, :HD], now[:, HD:])

        @pl.loop(0, n)
        def _(e):
            block_copy(slot, 0, e).wait()

        @each_chunk(1)
        def _(c):
            s = score(chunk_start(c))
            codes = []
            for p in range(blocks):
                e = (c - 1) * 4 + p
                codes.append(jnp.where(e < n, plan[b, e] // 256, 0))
            for i in range(blocks):
                shift = jnp.zeros((1, CHUNK), jnp.float32)
                for p in range(blocks):
                    absent = jnp.where((codes[p] >> i) & 1 != 0, jnp.float32(0), -jnp.inf)
                    shift = jnp.where(place == p, absent, shift)
                for h in range(heads):
                    now = s[part(h, i)] + shift
                    scores[c, part(h, i), :] = now
                    high[part(h, i), :] = jnp.maximum(high[part(h, i), :], jnp.maximum(now[:, :HD], now[:, HD:]))

        for h in range(heads):
            for i in range(blocks):
                top = jnp.max(high[part(h, i), :], axis=1, keepdims=True)
                high[part(h, i), :] = jnp.broadcast_to(top, (KB, HD))
        total[...] = jnp.zeros_like(total)

        @each_chunk(0)
        def _(c):
            for h in range(heads):
                for i in range(blocks):
                    top = high[part(h, i), :]
                    left = jnp.exp(scores[c, part(h, i), :HD] - top)
                    right = jnp.exp(scores[c, part(h, i), HD:] - top)
                    scores[c, part(h, i), :HD] = left
                    scores[c, part(h, i), HD:] = right
                    total[part(h, i), :] += left + right

        again = jnp.int32(0)
        for i in range(blocks):
            again += plan[MORE + b * 4 + i, REPEATS]

        def self_part(h, i):
            return jnp.where(col == row + i * KB, scores[0, part(h, i), :], 0.0)

        @pl.when(again > 0)
        def _():
            for h in range(heads):
                for i in range(blocks):
                    e = self_part(h, i)
                    times = plan[MORE + b * 4 + i, REPEATS].astype(jnp.float32)
                    total[part(h, i), :] += times * (e[:, :HD] + e[:, HD:])

        for h in range(heads):
            for i in range(blocks):
                share = 1.0 / jnp.sum(total[part(h, i), :], axis=1, keepdims=True)
                total[part(h, i), :] = jnp.broadcast_to(share, (KB, HD))
        acc[...] = jnp.zeros_like(acc)

        @pl.when(again > 0)
        def _():
            for h in range(heads):
                for i in range(blocks):
                    share = total[part(h, i), :]
                    e = self_part(h, i)
                    weight = jnp.concatenate([e[:, :HD] * share, e[:, HD:] * share], axis=1)
                    times = plan[MORE + b * 4 + i, REPEATS].astype(jnp.float32)
                    acc[part(h, i), :] = times * jnp.dot(
                        weight.astype(jnp.bfloat16), held[:SPAN, HD:], preferred_element_type=jnp.float32)

        @each_chunk(0)
        def _(c):
            share = total[...]
            weight = jnp.concatenate([scores[c, :, :HD] * share, scores[c, :, HD:] * share], axis=1)
            acc[...] += jnp.dot(weight.astype(jnp.bfloat16),
                                held[pl.ds(chunk_start(c), CHUNK), HD:],
                                preferred_element_type=jnp.float32)

        pos = kv * SPAN + lax.broadcasted_iota(jnp.int32, (SPAN, HD), 0)
        for h in range(heads):
            done = jnp.where(pos < lengths[b], acc[h * SPAN:(h + 1) * SPAN, :], 0.0)
            out[slot, :, h * HD:(h + 1) * HD] = done.astype(jnp.bfloat16)

    load_q = pltpu.make_async_copy(q_in, q, q_sem)
    load_q.start()

    @pl.when(slots > 0)
    def _():
        fetch(jnp.int32(0))

    @pl.loop(slots, SEQS)
    def _(slot):
        out[slot] = jnp.zeros((SPAN, 2 * HD), jnp.bfloat16)

    load_q.wait()

    @pl.loop(0, slots)
    def _(slot):
        @pl.when(slot + 1 < slots)
        def _():
            fetch(slot + 1)

        compute(slot)


def attend(lengths, plan, q, cache):
    most = NZ * NX * (SPAN // KB)
    rows = 2 * SPAN
    return pl.pallas_call(
        attend_kernel,
        name="attend",
        out_shape=jax.ShapeDtypeStruct((SEQS, SPAN, 2 * HD), jnp.bfloat16),
        in_specs=[SMEM, SMEM, ANY, ANY],
        out_specs=VMEM,
        scratch_shapes=[
            pltpu.VMEM((SEQS, SPAN, 2 * HD), jnp.bfloat16),
            pltpu.VMEM((2, SPAN + most * KB, 2 * HD), jnp.bfloat16),
            pltpu.VMEM((1 + most // 4, rows, CHUNK), jnp.float32),
            pltpu.VMEM((rows, HD), jnp.float32),
            pltpu.VMEM((rows, HD), jnp.float32),
            pltpu.VMEM((rows, HD), jnp.float32),
            pltpu.SemaphoreType.DMA,
            pltpu.SemaphoreType.DMA((2,)),
            pltpu.SemaphoreType.DMA((2,)),
        ],
    )(lengths, plan, q, cache)


def mix_kernel(reach, lengths, attended, columns_in, out_w, out, groups, own, columns, own_w, acc,
               load_sem, next_recv, prev_recv, core_recv, sent):
    kv, tp = lax.axis_index("kv"), lax.axis_index("tp")
    z = kv // NX
    y, core = tp // 2, tp % 2
    y_next, y_prev, y_far = (y + 1) % NY, (y + NY - 1) % NY, (y + 2) % NY
    after, before = {"tp": y_next * 2 + core}, {"tp": y_prev * 2 + core}
    partner = {"tp": y * 2 + 1 - core}
    half = SPAN // 2

    barrier = pltpu.get_barrier_semaphore()
    for d in (after, before, partner):
        pl.semaphore_signal(barrier, inc=1, device_id=d, device_id_type=MESH)
    my_columns = out_w.at[:, pl.ds(pl.multiple_of(tp * SPAN, SPAN), SPAN)]
    loads = (
        pltpu.make_async_copy(attended, own, load_sem.at[0]),
        pltpu.make_async_copy(my_columns, own_w, load_sem.at[1]),
        pltpu.make_async_copy(columns_in, columns, load_sem.at[2]),
    )
    for load in loads:
        load.start()
    loads[0].wait()
    pl.semaphore_wait(barrier, 3)

    def piece(owner_y, owner_core, slot, h):
        return groups.at[owner_y * 2 + owner_core, slot, pl.ds(h * half, half)]

    def copy(src, dst, send_sem, recv_sem, device):
        return pltpu.make_async_remote_copy(
            src_ref=src, dst_ref=dst, send_sem=send_sem, recv_sem=recv_sem,
            device_id=device, device_id_type=MESH)

    def mine(slot, h):
        return own.at[slot, pl.ds(h * half, half)]

    def to_next(slot, h):
        return copy(mine(slot, h), piece(y, core, slot, h), sent.at[slot], next_recv.at[h, slot], after)

    def to_prev(slot, h):
        return copy(mine(slot, h), piece(y, core, slot, h), sent.at[slot], prev_recv.at[h, slot], before)

    def on_next(slot):
        here = piece(y_prev, core, slot, 0)
        return copy(here, here, sent.at[slot], next_recv.at[2, slot], after)

    def on_prev(slot):
        here = piece(y_next, core, slot, 1)
        return copy(here, here, sent.at[slot], prev_recv.at[2, slot], before)

    def across(stage, owner_y, slot, h, src=None):
        here = piece(owner_y, core, slot, h)
        return copy(here if src is None else src, here, sent.at[slot], core_recv.at[stage, slot], partner)

    def crossed(stage, slot):
        both = groups.at[0, slot]
        copy(both, both, sent.at[slot], core_recv.at[stage, slot], partner).wait_recv()

    def each(body):
        for slot in range(SEQS):
            @pl.when(z <= reach[slot])
            def _(slot=slot):
                body(slot)

    def product(rows, weight):
        part = jnp.dot(rows, weight, preferred_element_type=jnp.float32)
        return part.astype(jnp.bfloat16).astype(jnp.float32)

    def add(slot, owner_y, owner_core):
        g = owner_y * 2 + owner_core
        acc[slot] += product(groups[g, slot], columns[g])

    def begin(slot):
        to_next(slot, 0).start()
        to_prev(slot, 1).start()
        to_next(slot, 1).start()
        to_prev(slot, 0).start()
        for h in range(2):
            across(0, y, slot, h, mine(slot, h)).start()

    def first(slot):
        acc[slot] = product(own[slot], own_w[...])

    def relay(slot):
        to_next(slot, 0).wait_recv()
        on_next(slot).start()
        across(1, y_prev, slot, 0).start()
        to_prev(slot, 1).wait_recv()
        on_prev(slot).start()
        across(2, y_next, slot, 1).start()
        to_next(slot, 1).wait_recv()
        across(1, y_prev, slot, 1).start()
        to_prev(slot, 0).wait_recv()
        across(2, y_next, slot, 0).start()

    def near(slot):
        crossed(0, slot)
        for owner_y, owner_core in ((y, 1 - core), (y_prev, core), (y_next, core)):
            add(slot, owner_y, owner_core)

    def middle(slot):
        for stage, owner_y in ((1, y_prev), (2, y_next)):
            crossed(stage, slot)
            add(slot, owner_y, 1 - core)

    def far(slot):
        on_next(slot).wait_recv()
        across(3, y_far, slot, 0).start()
        on_prev(slot).wait_recv()
        across(3, y_far, slot, 1).start()
        if slot > 0:
            last(slot - 1)
        add(slot, y_far, core)

    def last(slot):
        crossed(3, slot)
        add(slot, y_far, 1 - core)

    def finish(slot):
        all_sent = groups.at[pl.ds(0, 7), slot]
        copy(all_sent, all_sent, sent.at[slot], core_recv.at[0, slot], partner).wait_send()

    each(begin)
    acc[...] = jnp.zeros_like(acc)
    loads[1].wait()
    each(first)
    loads[2].wait()

    def both(slot):
        relay(slot)
        near(slot)

    each(both)
    each(middle)
    each(far)
    for slot in range(SEQS):
        beyond = z <= reach[slot + 1] if slot + 1 < SEQS else z < 0

        @pl.when((z <= reach[slot]) & jnp.logical_not(beyond))
        def _(slot=slot):
            last(slot)

    for b in range(SEQS):
        slot = jnp.int32(0)
        for o in range(SEQS):
            if o < b:
                slot += (lengths[o] >= lengths[b]).astype(jnp.int32)
            elif o > b:
                slot += (lengths[o] > lengths[b]).astype(jnp.int32)
        out[b] = acc[slot].astype(jnp.bfloat16)
    each(finish)


def mix(reach, lengths, own, columns, out_weight):
    dma = pltpu.SemaphoreType.DMA
    return pl.pallas_call(
        lambda *refs: mix_kernel(reach, *refs),
        name="mix",
        out_shape=jax.ShapeDtypeStruct((SEQS, SPAN, SPAN), jnp.bfloat16),
        in_specs=[SMEM, ANY, ANY, ANY],
        out_specs=VMEM,
        scratch_shapes=[
            pltpu.VMEM((NTP, SEQS, SPAN, 2 * HD), jnp.bfloat16),
            pltpu.VMEM((SEQS, SPAN, 2 * HD), jnp.bfloat16),
            pltpu.VMEM((NTP, SPAN, SPAN), jnp.bfloat16),
            pltpu.VMEM((SPAN, SPAN), jnp.bfloat16),
            pltpu.VMEM((SEQS, SPAN, SPAN), jnp.float32),
            dma((3,)),
            dma((3, SEQS)),
            dma((3, SEQS)),
            dma((4, SEQS)),
            dma((SEQS,)),
        ],
        compiler_params=pltpu.CompilerParams(
            collective_id=2 if reach == REACH else 3, has_side_effects=True
        ),
    )(lengths, own, columns, out_weight)


def shards(inputs, query_weight, key_weight, value_weight, out_weight, chosen, lengths):
    def rest(reach):
        cache, columns, queries, plan = spread(
            reach, lengths, chosen, inputs, query_weight, key_weight, value_weight, out_weight)
        attended = attend(lengths, plan, queries, cache)
        return mix(reach, lengths, attended, columns, out_weight)

    score = jnp.where(lengths > 3072, 6, jnp.where(lengths > 2048, 3, jnp.where(lengths > 1024, 2, 0)))
    near = jnp.sum(score) < 12
    return lax.cond(near, lambda: rest(NEAR_REACH), lambda: rest(REACH))


def solution(mesh):
    placed = (
        P(None, "kv", None),
        P(None, "tp"),
        P(None, "tp"),
        P(None, "tp"),
        P("tp", None),
        P(None, "kv", None),
        P(),
    )
    return jax.shard_map(
        shards, mesh=mesh, in_specs=placed, out_specs=P(None, "kv", "tp"), check_vma=False
    )
```
